32 devices in a mesh: grp: 2 (over y), sp: 4 (over z), tp: 4 (over x, core).
Axes of the slice: x: 2, y: 2, z: 4, core: 2. Of those that a mesh axis runs over, the one named last changes fastest.
Arguments:
- carryover_vector: bfloat16 [2048, 2048], P(('grp', 'sp', 'tp')), parts along dimension 0, may hold values from -6 to 6
- channel_source_entries: bfloat16 [2048, 1024], P(('grp', 'sp'), 'tp'), parts along dimension 0, may hold values from -6 to 6
- final_modulation_vector: bfloat16 [2048, 1024], P(('grp', 'sp'), 'tp'), parts along dimension 0, may hold values from -54 to 54
- entering_basis_matrix: bfloat16 [2048, 512], P(('grp', 'sp'), 'tp'), parts along dimension 0, may hold values from -6 to 6
- readout_basis_matrix: bfloat16 [2048, 512], P(('grp', 'sp'), 'tp'), parts along dimension 0, may hold values from -6 to 6
- raw_stride_amount: float32 [2048, 16], P(('grp', 'sp'), 'tp'), parts along dimension 0, may hold values from -6 to 5
- extra_log_attenuation: float32 [2048, 16], P(('grp', 'sp'), 'tp'), parts along dimension 0, may hold values from -1.4 to 0
- channel_fading_rate: float32 [16], P('tp'), may hold values from 0 to 0.1, as said below
- channel_source_kernel: float32 [4, 1024], P(None, 'tp'), may hold values from -3 to 3
- entering_basis_kernel: float32 [4, 512], P(None, 'tp'), may hold values from -3 to 3
- readout_basis_kernel: float32 [4, 512], P(None, 'tp'), may hold values from -3 to 3
- modulated_rescaling_vector: float32 [1024], replicated, may hold values from 0.1 to 1.9
- blender_final_matrix: bfloat16 [1024, 2048], replicated, may hold values from -0.1875 to 0.1875
- specialist_rescaling_vector: float32 [2048], replicated, may hold values from 0.1 to 1.9
- specialist_gating_matrices: bfloat16 [8, 2048, 1024], P('sp', None, 'tp'), may hold values from -0.125 to 0.125
- widening_matrices: bfloat16 [8, 2048, 1024], P('sp', None, 'tp'), may hold values from -0.125 to 0.125
- contracting_matrices: bfloat16 [8, 1024, 2048], P('sp', 'tp'), may hold values from -0.1875 to 0.1875
- assigned_specialist_ids: int32 [2048, 2], P(('grp', 'sp')), parts along dimension 0, may hold values from 0 to 7, as said below
- specialist_choice_affinity: float32 [2048, 2], P(('grp', 'sp', 'tp')), parts along dimension 0, may hold values from -6 to 6
- cluster_chance: float32 [2048], P(('grp', 'sp', 'tp')), parts along dimension 0, may hold values from 0.25 to 1
Outputs:
- layer_out: bfloat16 [2048, 2048], P(('grp', 'sp', 'tp')), parts along dimension 0
The draws below stay inside these ranges and needn't reach their ends.
There are 2 independent parts, one for each index of `grp`. The reference program is written for one: setup_inputs(seed, part) draws one part's arguments, and reference() takes and returns one part's arrays. A program takes and returns all parts, laid end to end along the dimension named above; an argument that names none is the same for every part. Nothing has to cross between parts.
Inputs may be any that keep to these rules, and one draw needn't show every extreme that they name: `assigned_specialist_ids`: each row names 2 different experts of one group: the experts g * 2 to (g + 1) * 2 - 1 for one g below 4. In each aligned block of 64 rows (the rows of one device) no expert is named by more than 32 rows, and every expert of one group, the same group in all blocks, is named by exactly 32 rows of every block. `channel_fading_rate`: positive.
All inputs are finite; a program needn't handle non-finite values.
Results may differ from the reference program's by a relative error of at most 0.015.
Values may be sent and summed in bfloat16 or wider, within the bound.
A program may use at most 64 MiB of HBM per device.

```python
import jax
import jax.numpy as jnp
from jax import lax

D = 2048
HEADS = 16
HEAD_DIM = 64
GROUPS_BC = 4
STATE = 128
CONV = 4
BLOCK = 64
FF = 1024
EGROUPS = 4
TOPK = 2
SEG_TOK = 256
D_SSD = 1024
ROWS = 64
TOKENS = 1024
EXPERTS = 8
CAP = 32
N_TP = 4


def draw_final_modulation_vector(key, part):
    row_key, column_key, base_key = jax.random.split(jax.random.fold_in(key, 7), 3)
    row_scale = jnp.exp(jax.random.uniform(row_key, (TOKENS, 1), jnp.float32, jnp.log(0.3), jnp.log(3.0)))
    column = jnp.arange(D_SSD, dtype=jnp.float32)[None, :] / D_SSD
    jitter = jnp.exp(jax.random.uniform(column_key, (1, D_SSD), jnp.float32, jnp.log(0.6), jnp.log(1.5)))
    base = jnp.clip(jax.random.normal(base_key, (TOKENS, D_SSD), jnp.float32), -4.0, 4.0)
    column_scale = jnp.exp(column * jnp.log(3.0)) * jitter
    return (base * row_scale * column_scale).astype(jnp.bfloat16)


def draw_raw_stride_amount(key, part):
    jitter_key, level_key = jax.random.split(jax.random.fold_in(key, 11))
    segments = TOKENS // SEG_TOK
    levels = jax.random.uniform(level_key, (segments, 1, 1), jnp.float32, -1.5, 1.0)
    jitter = jnp.clip(jax.random.normal(jitter_key, (segments, SEG_TOK, HEADS), jnp.float32), -4.5, 4.0)
    return (jitter + levels).reshape(TOKENS, HEADS)


def draw_channel_fading_rate(key, part):
    pick_key, slow_key, fast_key = jax.random.split(jax.random.fold_in(key, 13), 3)
    slow_share = 0.5
    is_slow = jax.random.uniform(pick_key, (HEADS,), jnp.float32) < slow_share
    slow_rates = jnp.exp(jax.random.uniform(slow_key, (HEADS,), jnp.float32, jnp.log(0.1 / TOKENS), jnp.log(1.0 / TOKENS)))
    fast_rates = jnp.exp(jax.random.uniform(fast_key, (HEADS,), jnp.float32, jnp.log(0.03), jnp.log(0.1)))
    return jnp.where(is_slow, slow_rates, fast_rates)


def draw_extra_log_attenuation(key, part):
    place_key, strength_key = jax.random.split(jax.random.fold_in(key, 17))
    places = jax.random.randint(place_key, (2, 1, HEADS), 0, TOKENS)
    strengths = jax.random.uniform(strength_key, (2, 1, HEADS), jnp.float32, 0.22, 0.69)
    positions = jnp.arange(TOKENS, dtype=jnp.int32)[None, :, None]
    return -jnp.sum(jnp.where(positions == places, strengths, 0.0), axis=0)


def draw_assigned_specialist_ids(key, part):
    blocks = TOKENS // ROWS
    per_group = EXPERTS // EGROUPS
    busy_rows = CAP * per_group // TOPK
    busy_key, other_key, order_key, deal_key = jax.random.split(jax.random.fold_in(key, 19), 4)
    busy_group = jax.random.randint(busy_key, (), 0, EGROUPS)
    others = jax.random.randint(other_key, (blocks, ROWS - busy_rows), 0, EGROUPS - 1)
    others = others + (others >= busy_group).astype(jnp.int32)
    groups = jnp.concatenate([jnp.full((blocks, busy_rows), busy_group, jnp.int32), others], axis=1)
    orders = jax.vmap(lambda subkey: jax.random.permutation(subkey, ROWS))(jax.random.split(order_key, blocks))
    groups = jnp.take_along_axis(groups, orders, axis=1)
    member = (groups[..., None] == jnp.arange(EGROUPS, dtype=jnp.int32)).astype(jnp.int32)
    ranking = jnp.sum((jnp.cumsum(member, axis=1) - member) * member, axis=2)
    dealing = jax.vmap(lambda subkey: jax.random.permutation(subkey, per_group))(jax.random.split(deal_key, blocks * EGROUPS)).reshape(blocks, EGROUPS, per_group)
    chosen = dealing[jnp.arange(blocks)[:, None], groups]
    first_place = TOPK * ranking % per_group
    first_pick = jnp.take_along_axis(chosen, first_place[..., None], axis=2)[..., 0]
    second_pick = jnp.take_along_axis(chosen, (first_place + 1)[..., None], axis=2)[..., 0]
    group_base = groups * per_group
    picked = jnp.stack([group_base + first_pick, group_base + second_pick], axis=-1)
    return picked.reshape(TOKENS, TOPK).astype(jnp.int32)


def block_levels(own_key, extent, cuts, low, top_value):
    def one(position, parts):
        steps = jax.random.uniform(jax.random.fold_in(jax.random.fold_in(own_key, 6), position), (parts,), jnp.float32, low / len(cuts), top_value / len(cuts))
        return jnp.repeat(jnp.exp(steps), extent[position] // parts).reshape((-1,) + (1,) * (len(extent) - position - 1))

    level = one(*cuts[0])
    for cut in cuts[1:]:
        level = level * one(*cut)
    return level


def centred(own_key, shape, width, limit, shards=(), kind=jnp.bfloat16):
    values = jax.random.normal(own_key, shape, jnp.float32) * width
    if len(shards) > 0:
        values = block_levels(own_key, shape, shards, -0.22, 0.18) * values
    return jnp.clip(values, min=-limit, max=limit).astype(kind)


def setup_inputs(seed: int = 0, part: int = 0) -> dict:
    streams_of = jax.random.split(jax.random.key(seed), 21)
    own_keys = jax.random.split(jax.random.fold_in(streams_of[20], part), 21)
    carryover_vector = centred(own_keys[0], (TOKENS, D), 1.0, 6.0, ((0, 16),))
    channel_source_entries = centred(own_keys[1], (TOKENS, D_SSD), 1.0, 6.0, ((0, 4), (1, 4)))
    final_modulation_vector = draw_final_modulation_vector(jax.random.fold_in(jax.random.fold_in(streams_of[20], part), 71), part)
    entering_basis_matrix = centred(own_keys[3], (TOKENS, GROUPS_BC * STATE), 1.0, 6.0, ((0, 4), (1, 4)))
    readout_basis_matrix = centred(own_keys[4], (TOKENS, GROUPS_BC * STATE), 1.0, 6.0, ((0, 4), (1, 4)))
    raw_stride_amount = draw_raw_stride_amount(jax.random.fold_in(jax.random.fold_in(streams_of[20], part), 71), part)
    extra_log_attenuation = draw_extra_log_attenuation(jax.random.fold_in(jax.random.fold_in(streams_of[20], part), 71), part)
    channel_fading_rate = draw_channel_fading_rate(jax.random.fold_in(streams_of[20], 71), part)
    channel_source_kernel = centred(streams_of[8], (CONV, D_SSD), CONV ** -0.5, 3.0, ((1, 4),), jnp.float32)
    entering_basis_kernel = centred(streams_of[9], (CONV, GROUPS_BC * STATE), CONV ** -0.5, 3.0, ((1, 4),), jnp.float32)
    readout_basis_kernel = centred(streams_of[10], (CONV, GROUPS_BC * STATE), CONV ** -0.5, 3.0, ((1, 4),), jnp.float32)
    modulated_rescaling_vector = jnp.clip(1.0 + 0.18 * jax.random.normal(streams_of[11], (D_SSD,), jnp.float32), 0.1, 1.9)
    blender_final_matrix = centred(streams_of[12], (D_SSD, D), D_SSD ** -0.5, 0.1875)
    specialist_rescaling_vector = jnp.clip(1.0 + 0.18 * jax.random.normal(streams_of[13], (D,), jnp.float32), 0.1, 1.9)
    specialist_gating_matrices = centred(streams_of[14], (EXPERTS, D, FF), D ** -0.5, 0.125, ((0, 4), (2, 4)))
    widening_matrices = centred(streams_of[15], (EXPERTS, D, FF), D ** -0.5, 0.125, ((0, 4), (2, 4)))
    contracting_matrices = centred(streams_of[16], (EXPERTS, FF, D), FF ** -0.5, 0.1875, ((0, 4), (1, 4)))
    assigned_specialist_ids = draw_assigned_specialist_ids(jax.random.fold_in(jax.random.fold_in(streams_of[20], part), 71), part)
    specialist_choice_affinity = centred(own_keys[18], (TOKENS, TOPK), 1.5, 6.0, ((0, 16),), jnp.float32)
    cluster_chance = jnp.clip(0.25 + 0.75 * jax.random.uniform(own_keys[19], (TOKENS,), jnp.float32) ** block_levels(own_keys[19], (TOKENS,), ((0, 16),), -0.2, 0.2), 0.25, 1.0)
    return dict(carryover_vector=carryover_vector, channel_source_entries=channel_source_entries, final_modulation_vector=final_modulation_vector, entering_basis_matrix=entering_basis_matrix, readout_basis_matrix=readout_basis_matrix, raw_stride_amount=raw_stride_amount, extra_log_attenuation=extra_log_attenuation, channel_fading_rate=channel_fading_rate, channel_source_kernel=channel_source_kernel, entering_basis_kernel=entering_basis_kernel, readout_basis_kernel=readout_basis_kernel, modulated_rescaling_vector=modulated_rescaling_vector, blender_final_matrix=blender_final_matrix, specialist_rescaling_vector=specialist_rescaling_vector, specialist_gating_matrices=specialist_gating_matrices, widening_matrices=widening_matrices, contracting_matrices=contracting_matrices, assigned_specialist_ids=assigned_specialist_ids, specialist_choice_affinity=specialist_choice_affinity, cluster_chance=cluster_chance)


EPS = 1e-06
HIGHEST = lax.Precision.HIGHEST

def causal_conv(signal, weights):
    kernel_len = weights.shape[0]
    length = signal.shape[0]
    padded = jnp.pad(signal.astype(jnp.float32), ((kernel_len - 1, 0), (0, 0)))
    accumulated = jnp.zeros((length, signal.shape[1]), jnp.float32)
    for offset in range(kernel_len):
        accumulated = accumulated + weights[offset][None, :] * padded[offset:offset + length]
    return jax.nn.silu(accumulated)

def state_space(scaled_in, log_attenuation, keys_b, queries_c):
    blocks = scaled_in.shape[0] // BLOCK
    per_group = HEADS // GROUPS_BC
    scaled_in = scaled_in.reshape(blocks, BLOCK, GROUPS_BC, per_group, HEAD_DIM)
    log_attenuation = log_attenuation.reshape(blocks, BLOCK, GROUPS_BC, per_group)
    keys_b = keys_b.reshape(blocks, BLOCK, GROUPS_BC, STATE)
    queries_c = queries_c.reshape(blocks, BLOCK, GROUPS_BC, STATE)
    lower_mask = jnp.tril(jnp.ones((BLOCK, BLOCK), dtype=bool))

    def advance(carried, pieces):
        block_in, block_log, block_b, block_c = pieces
        running = jnp.cumsum(block_log, axis=0)
        between = running[:, None] - running[None, :]
        decays = jnp.exp(jnp.where(lower_mask[:, :, None, None], between, -jnp.inf))
        scores = jnp.einsum('lgn,sgn->lsg', block_c, block_b, precision=HIGHEST)
        inside = jnp.einsum('lsg,lsgr,sgrp->lgrp', scores, decays, block_in, precision=HIGHEST)
        outside = jnp.einsum('lgn,grpn,lgr->lgrp', block_c, carried, jnp.exp(running), precision=HIGHEST)
        remain = jnp.exp(running[-1][None] - running)
        updated = carried * jnp.exp(running[-1])[:, :, None, None] + jnp.einsum('sgn,sgr,sgrp->grpn', block_b, remain, block_in, precision=HIGHEST)
        return (updated, inside + outside)
    initial = jnp.zeros((GROUPS_BC, per_group, HEAD_DIM, STATE), jnp.float32)
    _, outputs = lax.scan(advance, initial, (scaled_in, log_attenuation, keys_b, queries_c))
    return outputs.reshape(blocks * BLOCK, HEADS, HEAD_DIM)

def reference(carryover_vector, channel_source_entries, final_modulation_vector, entering_basis_matrix, readout_basis_matrix, raw_stride_amount, extra_log_attenuation, channel_fading_rate, channel_source_kernel, entering_basis_kernel, readout_basis_kernel, modulated_rescaling_vector, blender_final_matrix, specialist_rescaling_vector, specialist_gating_matrices, widening_matrices, contracting_matrices, assigned_specialist_ids, specialist_choice_affinity, cluster_chance):
    length = carryover_vector.shape[0]
    inputs_x = causal_conv(channel_source_entries, channel_source_kernel)
    keys_b = causal_conv(entering_basis_matrix, entering_basis_kernel)
    queries_c = causal_conv(readout_basis_matrix, readout_basis_kernel)
    channel_stride_amount = jax.nn.softplus(raw_stride_amount)
    log_attenuation = extra_log_attenuation - channel_fading_rate[None, :] * channel_stride_amount
    heads_x = inputs_x.reshape(length, HEADS, HEAD_DIM)
    mixed = state_space(heads_x * channel_stride_amount[:, :, None], log_attenuation, keys_b, queries_c)
    gated = mixed.reshape(length, D_SSD) * jax.nn.silu(final_modulation_vector.astype(jnp.float32))
    normed = (gated * lax.rsqrt(lax.optimization_barrier(jnp.mean(gated * gated, axis=1, keepdims=True)) + EPS) * modulated_rescaling_vector[None, :]).astype(jnp.bfloat16)
    middle = (carryover_vector.astype(jnp.float32) + jnp.dot(normed, blender_final_matrix, preferred_element_type=jnp.float32)).astype(jnp.bfloat16)
    middle_wide = middle.astype(jnp.float32)
    expert_input = (middle_wide * lax.rsqrt(lax.optimization_barrier(jnp.mean(middle_wide * middle_wide, axis=1, keepdims=True)) + EPS) * specialist_rescaling_vector[None, :]).astype(jnp.bfloat16)
    assigned = assigned_specialist_ids.reshape(-1)
    count_all = assigned.shape[0]
    member = (assigned[:, None] == jnp.arange(EXPERTS, dtype=jnp.int32)[None, :]).astype(jnp.int32)
    ranking = lax.optimization_barrier(jnp.sum((jnp.cumsum(member, axis=0) - member) * member, axis=1))
    slot_count = length // ROWS * CAP
    table = jnp.full((EXPERTS, slot_count), -1, jnp.int32).at[assigned, ranking].set(jnp.arange(count_all, dtype=jnp.int32))
    lifted = jnp.exp(specialist_choice_affinity)
    shares = (cluster_chance[:, None] * lifted / lax.optimization_barrier(jnp.sum(lifted, axis=1, keepdims=True))).reshape(-1)
    quarter = FF // N_TP

    def expert_pass(combined, expert_index):
        slot_ids = table[expert_index]
        is_live = slot_ids >= 0
        safe_ids = jnp.maximum(slot_ids, 0)
        token_ids = safe_ids // TOPK
        chosen = jnp.take(expert_input, token_ids, axis=0)
        gate_value = jnp.dot(chosen, specialist_gating_matrices[expert_index], preferred_element_type=jnp.float32)
        up_value = jnp.dot(chosen, widening_matrices[expert_index], preferred_element_type=jnp.float32)
        hidden = (jax.nn.silu(gate_value) * up_value).astype(jnp.bfloat16)
        down_rows = contracting_matrices[expert_index]
        summed = jnp.zeros((slot_count, D), jnp.float32)
        for part_index in range(N_TP):
            piece_sum = jnp.dot(hidden[:, part_index * quarter:(part_index + 1) * quarter], down_rows[part_index * quarter:(part_index + 1) * quarter], preferred_element_type=jnp.float32).astype(jnp.bfloat16)
            summed = summed + lax.optimization_barrier(piece_sum).astype(jnp.float32)
        result = lax.optimization_barrier(summed.astype(jnp.bfloat16)).astype(jnp.float32)
        weight_column = jnp.where(is_live, shares[safe_ids], 0.0)
        return (combined.at[token_ids].add(weight_column[:, None] * result), None)
    combined, _ = lax.scan(expert_pass, jnp.zeros((length, D), jnp.float32), jnp.arange(EXPERTS, dtype=jnp.int32))
    return (middle_wide + combined).astype(jnp.bfloat16)
```

```python
import functools

import jax
import jax.numpy as jnp
from jax import lax
from jax.experimental import pallas as pl
from jax.experimental.pallas import tpu as pltpu
from jax.sharding import PartitionSpec as P

HEAD_DIM = 64
STATE = 128
EXPERT_GROUPS = 4
EPS = 1e-06
HIGHEST = lax.Precision.HIGHEST
F32 = jnp.float32
BF16 = jnp.bfloat16
TAIL = 16
EXTRA = 128


def silu(v):
    return v / (1.0 + jnp.exp(-v))


def iota(shape, dim):
    return lax.broadcasted_iota(jnp.int32, shape, dim)


def first_dims(a, b, precision=None):
    return lax.dot_general(
        a, b, (((0,), (0,)), ((), ())), precision=precision, preferred_element_type=F32
    )


def last_dims(a, b):
    return lax.dot_general(
        a, b, (((1,), (1,)), ((), ())), precision=HIGHEST, preferred_element_type=F32
    )


def spread(cols, width):
    heads = cols.shape[1]
    lane_head = iota((cols.shape[0], width), 1) // HEAD_DIM
    out = jnp.broadcast_to(cols[:, 0:1], (cols.shape[0], width))
    for h in range(1, heads):
        out = jnp.where(lane_head == h, cols[:, h : h + 1], out)
    return out


def members(ids, n, locals_):
    count = -(-n // 8) * 8
    low = iota((count, ids.shape[1]), 0) * locals_
    id0, id1 = ids[0:1], ids[1:2]
    hit0 = (id0 >= low) & (id0 < low + locals_)
    hit1 = (id1 >= low) & (id1 < low + locals_)
    return jnp.where(hit0, 1.0, 0.0), jnp.where(hit0 | hit1, 1.0, 0.0)


def places(hit, rows):
    length = hit.shape[1]
    i, j = iota((length, length), 0), iota((length, length), 1)
    earlier = jnp.where((i < j) & (i // rows == j // rows), 1.0, 0.0).astype(BF16)
    return jnp.dot(hit.astype(BF16), earlier, preferred_element_type=F32)


def kernel(n, tp, cap, names, *refs):
    r = dict(zip(names, refs))
    s = lax.axis_index("sp")
    t = lax.axis_index("tp")
    length, width = r["x"].shape
    rows, model = r["carry"].shape
    heads = width // HEAD_DIM
    locals_ = r["wg"].shape[0]
    slots = tp * cap
    far = (t + tp // 2) % tp
    near = t + 1 - 2 * (t % 2)
    near_far = (near + tp // 2) % tp

    if n == 4:
        half = s // 2
        own = 0
        source = [
            s,
            half + (1 - half) * (1 - s),
            2 * (1 - half) + half * (5 - s),
            3 * (1 - half),
        ]
        routes = ([1, 2, 3], [2, 3, 0], [1, 0, 3], [2, 1, 0])
    else:
        own = s
        routes = [[d for d in range(n) if d != v] for v in range(n)]

    def source_of(j):
        return source[j] if n == 4 else j

    def early(v):
        return [("c", d) for d in (routes[v][:1] if v == 0 and n == 4 else routes[v])]

    def late(v):
        return [("g", d) for d in (routes[v][:1] if v == 0 and n == 4 else routes[v])]

    def last(v):
        return [("c", 3), ("g", 3), ("c", 2), ("g", 2)] if v == 0 and n == 4 else []

    def slot_at(d):
        if n != 4:
            return s
        if d < 2:
            return half * s + 1 - half
        return (1 - half) * (3 - 2 * s) + 2 * half

    def remote(src, dst, ssem, rsem, sp, tpi):
        return pltpu.make_async_remote_copy(
            src_ref=src,
            dst_ref=dst,
            send_sem=ssem,
            recv_sem=rsem,
            device_id={"sp": sp, "tp": tpi},
            device_id_type=pl.DeviceIdType.MESH,
        )

    barrier = pltpu.get_barrier_semaphore()
    peers = [((s + k) % n, t) for k in range(1, n)] + [(s, near), (s, far)]
    for sp, tpi in peers:
        pl.semaphore_signal(
            barrier,
            inc=1,
            device_id={"sp": sp, "tp": tpi},
            device_id_type=pl.DeviceIdType.MESH,
        )
    fetches = {}
    for i, name in enumerate(INPUTS):
        fetches[name] = pltpu.make_async_copy(r[name + "_hbm"], r[name], r["local_sem"].at[i])
        fetches[name].start()

    def fetched(*wanted):
        for name in wanted:
            fetches[name].wait()

    fetched("x", "b", "c")

    with jax.named_scope("barrier"):
        pl.semaphore_wait(barrier, len(peers))

    tails = []
    for i, name in enumerate("xbc"):
        copy = remote(
            r[name].at[pl.ds(length - TAIL, TAIL)],
            r["tail_" + name],
            r["tail_ss"].at[i],
            r["tail_rs"].at[i],
            (s + 1) % n,
            t,
        )
        copy.start()
        tails.append(copy)


    landing = {"c": r["carr"], "g": r["gbuf"]}

    def crossing(kind, d, place):
        return remote(
            r[kind + "_send"].at[d],
            landing[kind].at[place, t],
            r[kind + "z_ss"].at[d],
            r[kind + "z_rs"].at[place],
            d,
            t,
        )

    def dispatch(kind, d):
        crossing(kind, d, slot_at(d)).start()

    def dispatches(plan):
        for v in range(n):
            if plan(v):

                @pl.when(s == v)
                def _(v=v):
                    for kind, d in plan(v):
                        dispatch(kind, d)

    def across(kind, j):
        ref = landing[kind]
        return remote(
            ref.at[j, t], ref.at[j, t], r[kind + "f_ss"].at[j], r[kind + "f_rs"].at[j], s, far
        )

    def beside(kind, j, i):
        ref = landing[kind]
        block = far if i else t
        return remote(
            ref.at[j, block],
            ref.at[j, block],
            r[kind + "n_ss"].at[j, i],
            r[kind + "n_rs"].at[j, i],
            s,
            near,
        )

    def spread_out(kind, j):
        across(kind, j).start()
        beside(kind, j, 0).start()

    def pass_far(kind, j):
        with jax.named_scope(f"z_{kind}"):
            crossing(kind, (s + 1) % n, j).wait_recv()
        spread_out(kind, j)

    def pass_near(kind, j):
        with jax.named_scope(f"far_{kind}"):
            across(kind, j).wait()
        beside(kind, j, 1).start()

    def gathered(kind, j):
        with jax.named_scope(f"near_{kind}"):
            beside(kind, j, 0).wait()
            beside(kind, j, 1).wait()

    fetched("ids", "aff", "chance")
    ids_all = r["ids"][...]
    ids = ids_all[:, 0:rows]
    for i in range(1, tp):
        ids = jnp.where(t == i, ids_all[:, i * rows : (i + 1) * rows], ids)
    first, hit = members(ids, n, locals_)
    place = places(hit, rows)
    lift = jnp.exp(r["aff"][...])
    share = r["chance"][...] / (lift[0:1] + lift[1:2])
    slot = iota((cap, rows), 0).astype(F32)
    lane = iota((cap, EXTRA), 1)
    fetched("carry")
    carry = r["carry"][...]
    for d in range(n):
        onehot = jnp.where((place[d : d + 1] == slot) & (hit[d : d + 1] > 0.5), 1.0, 0.0)
        r["oh_own"][d] = onehot.astype(BF16)
        r["c_send"][d, :, 0:model] = jnp.dot(
            onehot.astype(BF16), carry, preferred_element_type=F32
        ).astype(BF16)
        flag = jnp.sum(onehot * first[d : d + 1], axis=1, keepdims=True)
        extra = jnp.where(lane == 2 * locals_, flag, 0.0)
        for l in range(locals_):
            expert = d * locals_ + l
            mine = share * (
                jnp.where(ids[0:1] == expert, lift[0:1], 0.0)
                + jnp.where(ids[1:2] == expert, lift[1:2], 0.0)
            )
            col = jnp.sum(onehot * mine, axis=1, keepdims=True)
            high = col.astype(BF16).astype(F32)
            extra = jnp.where(lane == 2 * l, high, extra)
            extra = jnp.where(lane == 2 * l + 1, col - high, extra)
        r["c_send"][d, :, model : model + EXTRA] = extra.astype(BF16)
    r["carr"][own, t] = r["c_send"][s]

    dispatches(early)
    spread_out("c", own)

    fetched("raw", "extra", "fade")
    dt_t = jnp.log1p(jnp.exp(r["raw"][...]))
    fade = jnp.broadcast_to(r["fade"][...], (heads, heads))
    fade = jnp.where(iota((heads, heads), 0) == iota((heads, heads), 1), fade, 0.0)
    la_t = r["extra"][...] - jnp.sum(fade, axis=1, keepdims=True) * dt_t
    row_i = iota((length, length), 0)
    col_i = iota((length, length), 1)
    lower = row_i >= col_i
    cum = last_dims(jnp.where(lower, 1.0, 0.0), la_t)
    dt = last_dims(jnp.where(row_i == col_i, 1.0, 0.0), dt_t)
    cum_t = jnp.dot(
        la_t,
        jnp.where(row_i <= col_i, 1.0, 0.0),
        precision=HIGHEST,
        preferred_element_type=F32,
    )

    ext = r["ext"]
    ext[TAIL:, 0:width] = r["x"][...].astype(F32)
    ext[TAIL:, width : width + STATE] = r["b"][...].astype(F32)
    ext[TAIL:, width + STATE : width + 2 * STATE] = r["c"][...].astype(F32)
    fetched("kx", "kb", "kc")
    with jax.named_scope("tails"):
        for copy in tails:
            copy.wait()
    inside = s > 0
    ext[0:TAIL, 0:width] = jnp.where(inside, r["tail_x"][...].astype(F32), 0.0)
    ext[0:TAIL, width : width + STATE] = jnp.where(inside, r["tail_b"][...].astype(F32), 0.0)
    ext[0:TAIL, width + STATE : width + 2 * STATE] = jnp.where(
        inside, r["tail_c"][...].astype(F32), 0.0
    )

    def conv(taps, first, count):
        kernel_len = taps.shape[0]
        total = None
        for j in range(kernel_len):
            at = TAIL - kernel_len + 1 + j
            term = taps[j : j + 1, :] * ext[at : at + length, first : first + count]
            total = term if total is None else total + term
        return silu(total)

    keys = conv(r["kb"], width, STATE).astype(BF16)
    xdt = conv(r["kx"], 0, width) * spread(dt, width)
    tot = cum[length - 1 : length, :]
    remain = jnp.exp(tot - cum)
    state = first_dims(keys, (xdt * spread(remain, width)).astype(BF16))
    r["st_send"][...] = state.astype(BF16)
    r["tot_send"][...] = jnp.broadcast_to(spread(tot, width), r["tot_send"].shape)

    def total_copy(k):
        return remote(
            r["tot_send"],
            r["tot_buf"].at[k],
            r["tot_ss"].at[k],
            r["tot_rs"].at[k],
            (s + k) % n,
            t,
        )

    def state_copy(k):
        return remote(
            r["st_send"],
            r["st_buf"].at[k],
            r["st_ss"].at[k],
            r["st_rs"].at[k],
            (s + k) % n,
            t,
        )

    if n == 4:

        @pl.when(s == 2)
        def _():
            total_copy(1).start()

        @pl.when(s % 2 == 0)
        def _():
            state_copy(1).start()

    else:
        for k in range(1, n):

            @pl.when(s + k < n)
            def _(k=k):
                total_copy(k).start()
                state_copy(k).start()

    first, hit = members(ids_all, n, locals_)
    place = places(hit, rows)
    slot_row, slot_pos = iota((slots, length), 0), iota((slots, length), 1)
    same = slot_row // cap == slot_pos // rows
    slot = (slot_row % cap).astype(F32)
    for d in range(n):
        onehot = same & (place[d : d + 1] == slot) & (hit[d : d + 1] > 0.5)
        r["oh_seg"][d] = jnp.where(onehot, 1.0, 0.0).astype(BF16)
    queries = conv(r["kc"], width + STATE, STATE).astype(BF16)
    scores = lax.dot_general(
        queries, keys, (((1,), (1,)), ((), ())), preferred_element_type=F32
    )
    xdt_b = xdt.astype(BF16)
    lane_head = iota((length, width), 1) // HEAD_DIM
    mixed = jnp.zeros((length, width), F32)
    for h in range(heads):
        between = jnp.where(lower, cum[:, h : h + 1] - cum_t[h : h + 1, :], -1e30)
        weights = (scores * jnp.exp(between)).astype(BF16)
        chosen = jnp.where(lane_head == h, xdt_b, jnp.zeros_like(xdt_b))
        mixed = mixed + jnp.dot(weights, chosen, preferred_element_type=F32)
    reach = jnp.exp(spread(cum, width))
    fetched("z")
    modulation = silu(r["z"][...].astype(F32))

    if n == 4:

        @pl.when(s == 1)
        def _():
            pass_far("c", 1)

        @pl.when(s == 2)
        def _():
            pass_far("c", 1)
            pass_far("c", 2)

        @pl.when(s == 3)
        def _():
            pass_far("c", 2)
            pass_far("c", 1)

    incoming = r["incoming"]
    incoming[...] = jnp.zeros_like(incoming)
    if n == 4:

        @pl.when(s == 1)
        def _():
            with jax.named_scope("state"):
                state_copy(1).wait_recv()
            before = r["st_buf"][1].astype(F32)
            incoming[...] = before
            r["st_send"][...] = (before * jnp.exp(r["tot_send"][0:1, :]) + state).astype(BF16)
            state_copy(1).start()
            state_copy(2).start()

        @pl.when(s == 2)
        def _():
            with jax.named_scope("state"):
                state_copy(1).wait_recv()
            incoming[...] = r["st_buf"][1].astype(F32)

        @pl.when(s == 3)
        def _():
            with jax.named_scope("state"):
                total_copy(1).wait_recv()
                state_copy(1).wait_recv()
                state_copy(2).wait_recv()
            incoming[...] = r["st_buf"][2].astype(F32) * jnp.exp(
                r["tot_buf"][1, 0:1, :]
            ) + r["st_buf"][1].astype(F32)

    else:
        for k in range(n - 1, 0, -1):

            @pl.when(k <= s)
            def _(k=k):
                total_copy(k).wait_recv()
                state_copy(k).wait_recv()
                incoming[...] = incoming[...] * jnp.exp(r["tot_buf"][k, 0:1, :]) + r["st_buf"][
                    k
                ].astype(F32)

    outside = jnp.dot(queries, incoming[...].astype(BF16), preferred_element_type=F32)
    gated = ((mixed + outside * reach) * modulation).astype(BF16)
    for d in range(n):
        picked = jnp.dot(r["oh_seg"][d], gated, preferred_element_type=F32)
        r["g_send"][d] = picked.astype(BF16).reshape(slots, width)
    r["gbuf"][own, t] = r["g_send"][s]
    dispatches(late)
    spread_out("g", own)

    with jax.named_scope("weights"):
        fetched("gain", "sgain", "blend", "wg", "wu", "wd")

    def experts(j, between=None):
        gathered("c", j)
        gathered("g", j)
        squares = jnp.zeros((slots, 1), F32)
        for i in range(tp):
            piece = r["gbuf"][j, i].astype(F32)
            squares = squares + jnp.sum(piece * piece, axis=1, keepdims=True)
        scale = lax.rsqrt(squares / (tp * width) + EPS)
        rowsin = r["carr"][j].reshape(slots, model + EXTRA)
        projected = rowsin[:, 0:model].astype(F32)
        for i in range(tp):
            span = slice(i * width, (i + 1) * width)
            normed = (r["gbuf"][j, i].astype(F32) * scale * r["gain"][:, span]).astype(BF16)
            projected = projected + jnp.dot(
                normed, r["blend"][span, :], preferred_element_type=F32
            )
        middle = projected.astype(BF16)
        r["mid"][...] = middle.reshape(tp, cap, model)
        r["keep"][j] = r["mid"][t]
        wide = middle.astype(F32)
        tokens = (
            wide
            * lax.rsqrt(jnp.mean(wide * wide, axis=1, keepdims=True) + EPS)
            * r["sgain"][...]
        ).astype(BF16)
        lots = rowsin[:, model : model + EXTRA].astype(F32)
        total = None
        for l in range(locals_):
            part_share = lots[:, 2 * l : 2 * l + 1] + lots[:, 2 * l + 1 : 2 * l + 2]
            gate = jnp.dot(tokens, r["wg"][l], preferred_element_type=F32)
            up = jnp.dot(tokens, r["wu"][l], preferred_element_type=F32)
            hidden = (silu(gate) * up * part_share).astype(BF16)
            term = jnp.dot(hidden, r["wd"][l], preferred_element_type=F32)
            total = term if total is None else total + term
            if l == 0 and between is not None:
                between()
        r["part"][j] = total.astype(BF16).reshape(tp, cap, model)
        near_copy(j, 1).start()
        near_copy(j, 0).start()

    def near_copy(j, i):
        return remote(
            r["part"].at[j, near if i == 0 else near_far],
            r["rs1"].at[j, i],
            r["p1_ss"].at[j, i],
            r["p1_rs"].at[j, i],
            s,
            near,
        )

    def far_copy(j):
        return remote(
            r["far_send"].at[j], r["rs2"].at[j], r["p2_ss"].at[j], r["p2_rs"].at[j], s, far
        )

    def reduce_near(j):
        with jax.named_scope("p1"):
            near_copy(j, 1).wait()
            near_copy(j, 0).wait()
        r["far_send"][j] = (
            r["part"][j, far].astype(F32) + r["rs1"][j, 1].astype(F32)
        ).astype(BF16)
        far_copy(j).start()

    def returning(j, place):
        return remote(
            r["ret_send"].at[j],
            r["ret"].at[place],
            r["ret_ss"].at[j],
            r["ret_rs"].at[place],
            source_of(j),
            t,
        )

    def reduce_far(j):
        with jax.named_scope("p2"):
            far_copy(j).wait()
        flag = r["carr"][j, t][:, model : model + EXTRA].astype(F32)
        r["ret_send"][j] = (
            r["keep"][j].astype(F32) * flag[:, 2 * locals_ : 2 * locals_ + 1]
            + r["part"][j, t].astype(F32)
            + r["rs1"][j, 0].astype(F32)
            + r["rs2"][j].astype(F32)
        ).astype(BF16)

        @pl.when(source_of(j) == s)
        def _():
            r["ret"][s] = r["ret_send"][j]

        @pl.when(source_of(j) != s)
        def _():
            returning(j, s).start()

    if n == 4:

        @pl.when(s > 0)
        def _():
            pass_far("g", 1)

        pass_near("c", 0)
        pass_near("g", 0)

        @pl.when(s == 3)
        def _():
            pass_far("g", 2)

        @pl.when(s > 0)
        def _():
            pass_near("c", 1)
            pass_near("g", 1)

        @pl.when(s == 3)
        def _():
            pass_far("c", 3)
            pass_far("g", 3)

        experts(0)
        dispatches(last)

        @pl.when(s == 0)
        def _():
            pass_far("c", 1)
            pass_far("g", 1)
            pass_far("c", 2)
            pass_near("c", 1)
            pass_near("g", 1)

        @pl.when(s == 1)
        def _():
            pass_far("c", 2)

        @pl.when(s < 3)
        def _():
            pass_far("g", 2)
            pass_far("c", 3)

        @pl.when(s < 2)
        def _():
            pass_far("g", 3)

        experts(1, lambda: reduce_near(0))

        @pl.when(s == 2)
        def _():
            pass_far("g", 3)

        pass_near("c", 2)
        pass_near("g", 2)
        experts(2, lambda: reduce_near(1))

        pass_near("c", 3)
        pass_near("g", 3)
        reduce_near(2)
        reduce_far(0)
        experts(3, lambda: reduce_far(1))
        reduce_near(3)
        reduce_far(2)
        reduce_far(3)
    else:

        def one(j, carried):
            @pl.when(j != s)
            def _():
                pass_far("c", j)
                pass_far("g", j)

            pass_near("c", j)
            pass_near("g", j)
            experts(j)
            reduce_near(j)
            reduce_far(j)
            return carried

        lax.fori_loop(0, n, one, 0)

    result = jnp.zeros((rows, model), F32)
    for d in range(n):

        @pl.when(s != d)
        def _(d=d):
            with jax.named_scope(f"ret_{d}"):
                returning(0, d).wait_recv()

        result = result + first_dims(r["oh_own"][d], r["ret"][d])
    r["out"][...] = result.astype(BF16)

    for j in range(n):

        @pl.when(s != j)
        def _(j=j):
            crossing("c", j, 0).wait_send()
            crossing("g", j, 0).wait_send()

        @pl.when(source_of(j) != s)
        def _(j=j):
            returning(j, s).wait_send()

    if n == 4:

        @pl.when(s == 2)
        def _():
            total_copy(1).wait_send()

        @pl.when(s % 2 == 0)
        def _():
            state_copy(1).wait_send()

        @pl.when(s == 1)
        def _():
            state_copy(1).wait_send()
            state_copy(2).wait_send()

    else:
        for k in range(1, n):

            @pl.when(s + k < n)
            def _(k=k):
                total_copy(k).wait_send()
                state_copy(k).wait_send()


INPUTS = ("x", "b", "c", "ids", "aff", "chance", "carry", "raw", "extra", "fade")
INPUTS += ("kx", "kb", "kc", "z", "gain", "sgain", "blend", "wg", "wu", "wd")


def per_device(
    n,
    tp,
    carryover_vector,
    channel_source_entries,
    final_modulation_vector,
    entering_basis_matrix,
    readout_basis_matrix,
    raw_stride_amount,
    extra_log_attenuation,
    channel_fading_rate,
    channel_source_kernel,
    entering_basis_kernel,
    readout_basis_kernel,
    modulated_rescaling_vector,
    blender_final_matrix,
    specialist_rescaling_vector,
    specialist_gating_matrices,
    widening_matrices,
    contracting_matrices,
    assigned_specialist_ids,
    specialist_choice_affinity,
    cluster_chance,
):
    length, width = channel_source_entries.shape
    rows, model = carryover_vector.shape
    locals_ = specialist_gating_matrices.shape[0]
    experts = n * locals_
    picks = assigned_specialist_ids.shape[1]
    assert tp == 4 and picks == 2 and entering_basis_matrix.shape[1] == STATE
    per_expert = 2 * rows * picks // experts
    group_size = experts // EXPERT_GROUPS
    if group_size <= locals_:
        cap = locals_ * per_expert // picks
    else:
        cap = locals_ * per_expert
    cap = -(-min(cap, rows) // 16) * 16
    slots = tp * cap
    given = dict(
        ids=assigned_specialist_ids.T,
        aff=specialist_choice_affinity.T,
        chance=cluster_chance[None, :],
        carry=carryover_vector,
        raw=raw_stride_amount.T,
        extra=extra_log_attenuation.T,
        fade=channel_fading_rate[None, :],
        x=channel_source_entries,
        b=entering_basis_matrix,
        c=readout_basis_matrix,
        kx=channel_source_kernel,
        kb=entering_basis_kernel,
        kc=readout_basis_kernel,
        z=final_modulation_vector,
        gain=modulated_rescaling_vector[None, :],
        sgain=specialist_rescaling_vector[None, :],
        blend=blender_final_matrix,
        wg=specialist_gating_matrices,
        wu=widening_matrices,
        wd=contracting_matrices,
    )
    operands = [pltpu.with_memory_space_constraint(given[name], pltpu.HBM) for name in INPUTS]
    vmem = pltpu.VMEM
    dma = pltpu.SemaphoreType.DMA
    scratch = {name: vmem(given[name].shape, given[name].dtype) for name in INPUTS}
    scratch |= dict(
        tail_x=vmem((TAIL, width), BF16),
        tail_b=vmem((TAIL, STATE), BF16),
        tail_c=vmem((TAIL, STATE), BF16),
        ext=vmem((TAIL + length, width + 2 * STATE), F32),
        st_send=vmem((STATE, width), BF16),
        tot_send=vmem((8, width), F32),
        st_buf=vmem((n, STATE, width), BF16),
        tot_buf=vmem((n, 8, width), F32),
        incoming=vmem((STATE, width), F32),
        oh_own=vmem((n, cap, rows), BF16),
        oh_seg=vmem((n, slots, length), BF16),
        c_send=vmem((n, cap, model + EXTRA), BF16),
        carr=vmem((n, tp, cap, model + EXTRA), BF16),
        g_send=vmem((n, slots, width), BF16),
        gbuf=vmem((n, tp, slots, width), BF16),
        mid=vmem((tp, cap, model), BF16),
        keep=vmem((n, cap, model), BF16),
        part=vmem((n, tp, cap, model), BF16),
        rs1=vmem((n, 2, cap, model), BF16),
        far_send=vmem((n, cap, model), BF16),
        rs2=vmem((n, cap, model), BF16),
        ret_send=vmem((n, cap, model), BF16),
        ret=vmem((n, cap, model), BF16),
        local_sem=dma((len(INPUTS),)),
    )
    for name, shape in dict(
        tail=(3,),
        st=(n,),
        tot=(n,),
        cz=(n,),
        cf=(n,),
        cn=(n, 2),
        gz=(n,),
        gf=(n,),
        gn=(n, 2),
        p1=(n, 2),
        p2=(n,),
        ret=(n,),
    ).items():
        scratch[name + "_ss"] = dma(shape)
        scratch[name + "_rs"] = dma(shape)
    names = [name + "_hbm" for name in INPUTS] + ["out"] + list(scratch)
    return pl.pallas_call(
        functools.partial(kernel, n, tp, cap, names),
        out_shape=pltpu.VMEM((rows, model), BF16),
        in_specs=[pl.BlockSpec(memory_space=pltpu.HBM)] * len(operands),
        out_specs=pl.BlockSpec(memory_space=pltpu.VMEM),
        scratch_shapes=list(scratch.values()),
        compiler_params=pltpu.CompilerParams(
            collective_id=0,
            has_side_effects=True,
            vmem_limit_bytes=(40 if n <= 8 else 60) * 1024 * 1024,
        ),
    )(*operands)


def solution(mesh):
    return jax.shard_map(
        functools.partial(per_device, mesh.shape["sp"], mesh.shape["tp"]),
        mesh=mesh,
        in_specs=(
            P(("grp", "sp", "tp"), None),
            P(("grp", "sp"), "tp"),
            P(("grp", "sp"), "tp"),
            P(("grp", "sp"), "tp"),
            P(("grp", "sp"), "tp"),
            P(("grp", "sp"), "tp"),
            P(("grp", "sp"), "tp"),
            P("tp"),
            P(None, "tp"),
            P(None, "tp"),
            P(None, "tp"),
            P(),
            P(),
            P(),
            P("sp", None, "tp"),
            P("sp", None, "tp"),
            P("sp", "tp", None),
            P(("grp", "sp"), None),
            P(("grp", "sp", "tp"), None),
            P(("grp", "sp", "tp")),
        ),
        out_specs=P(("grp", "sp", "tp"), None),
        check_vma=False,
    )
```

```python
import functools

import jax
import jax.numpy as jnp
from jax import lax
from jax.experimental import pallas as pl
from jax.experimental.pallas import tpu as pltpu
from jax.sharding import PartitionSpec as P

HEAD_DIM = 64
STATE = 128
EXPERT_GROUPS = 4
EPS = 1e-06
HIGHEST = lax.Precision.HIGHEST
F32 = jnp.float32
BF16 = jnp.bfloat16
TAIL = 16
EXTRA = 128


def silu(v):
    return v / (1.0 + jnp.exp(-v))


def iota(shape, dim):
    return lax.broadcasted_iota(jnp.int32, shape, dim)


def first_dims(a, b, precision=None):
    return lax.dot_general(
        a, b, (((0,), (0,)), ((), ())), precision=precision, preferred_element_type=F32
    )


def last_dims(a, b):
    return lax.dot_general(
        a, b, (((1,), (1,)), ((), ())), precision=HIGHEST, preferred_element_type=F32
    )


def spread(cols, width):
    heads = cols.shape[1]
    lane_head = iota((cols.shape[0], width), 1) // HEAD_DIM
    out = jnp.broadcast_to(cols[:, 0:1], (cols.shape[0], width))
    for h in range(1, heads):
        out = jnp.where(lane_head == h, cols[:, h : h + 1], out)
    return out


def members(ids, n, locals_):
    count = -(-n // 8) * 8
    low = iota((count, ids.shape[1]), 0) * locals_
    id0, id1 = ids[0:1], ids[1:2]
    hit0 = (id0 >= low) & (id0 < low + locals_)
    hit1 = (id1 >= low) & (id1 < low + locals_)
    return jnp.where(hit0, 1.0, 0.0), jnp.where(hit0 | hit1, 1.0, 0.0)


def places(hit, rows):
    length = hit.shape[1]
    i, j = iota((length, length), 0), iota((length, length), 1)
    earlier = jnp.where((i < j) & (i // rows == j // rows), 1.0, 0.0).astype(BF16)
    return jnp.dot(hit.astype(BF16), earlier, preferred_element_type=F32)


def halves_of(cap):
    return 2 if cap % 32 == 0 else 1


def kernel(n, tp, cap, names, *refs):
    r = dict(zip(names, refs))
    s = lax.axis_index("sp")
    t = lax.axis_index("tp")
    length, width = r["x"].shape
    rows, model = r["carry"].shape
    heads = width // HEAD_DIM
    locals_ = r["wg"].shape[0]
    slots = tp * cap
    halves = halves_of(cap)
    part_rows = cap // halves
    far = (t + tp // 2) % tp
    near = t + 1 - 2 * (t % 2)
    near_far = (near + tp // 2) % tp

    place4 = (1 + 3 * (s % 2)) * (1 + 15 * (s // 2))

    def listed(row):
        return sum(v * 4**i for i, v in enumerate(row)) // place4 % 4

    if n == 4:
        own = 0
        source = [listed([ORDER[v][j] for v in range(n)]) for j in range(n)]
    else:
        own = s
        routes = [[d for d in range(n) if d != v] for v in range(n)]

    def source_of(j):
        return source[j] if n == 4 else j

    def planned(stage, v):
        if n == 4:
            return [("c" if code < G else "g", code % 10) for code in SENDS[v][stage]]
        return [("cg"[stage // 2], d) for d in routes[v]] if stage % 2 == 0 else []

    def slot_at(d):
        return listed([ORDER[d].index(v) for v in range(n)]) if n == 4 else s

    def remote(src, dst, ssem, rsem, sp, tpi):
        return pltpu.make_async_remote_copy(
            src_ref=src,
            dst_ref=dst,
            send_sem=ssem,
            recv_sem=rsem,
            device_id={"sp": sp, "tp": tpi},
            device_id_type=pl.DeviceIdType.MESH,
        )

    barrier = pltpu.get_barrier_semaphore()
    peers = [((s + k) % n, t) for k in range(1, n)] + [(s, near), (s, far)]
    if n == 4:
        peers.append((s + 1 - 2 * (s % 2), near))
    for sp, tpi in peers:
        pl.semaphore_signal(
            barrier,
            inc=1,
            device_id={"sp": sp, "tp": tpi},
            device_id_type=pl.DeviceIdType.MESH,
        )
    fetches = {}
    for i, name in enumerate(INPUTS):
        fetches[name] = pltpu.make_async_copy(r[name + "_hbm"], r[name], r["local_sem"].at[i])
        fetches[name].start()

    def fetched(*wanted):
        for name in wanted:
            fetches[name].wait()

    fetched("x", "b", "c")

    with jax.named_scope("barrier"):
        pl.semaphore_wait(barrier, len(peers))

    tail_lanes = dict(x=(0, width), b=(width, STATE), c=(width + STATE, STATE))
    for name, (first, count) in tail_lanes.items():
        r["tail_send"][:, first : first + count] = r[name][length - TAIL :, :]
    tails = remote(
        r["tail_send"], r["tail"], r["tail_ss"].at[0], r["tail_rs"].at[0], (s + 1) % n, t
    )

    @pl.when(s < n - 1)
    def _():
        tails.start()

    landing = {"c": r["carr"], "g": r["gbuf"]}

    def crossing(kind, d, place, lands=None):
        lands = d if lands is None else lands
        return remote(
            r[kind + "_send"].at[d],
            landing[kind].at[place, t],
            r[kind + "z_ss"].at[(d + n - 1 - s) % n],
            r[kind + "z_rs"].at[place - 1 if n == 4 else (place + n - 1 - lands) % n],
            d,
            t,
        )

    def dispatch(kind, d):
        crossing(kind, d, slot_at(d)).start()

    def dispatches(stage):
        for v in range(n):
            if planned(stage, v):

                @pl.when(s == v)
                def _(v=v):
                    for kind, d in planned(stage, v):
                        dispatch(kind, d)

    def across(kind, j):
        ref = landing[kind]
        return remote(
            ref.at[j, t], ref.at[j, t], r[kind + "f_ss"].at[j], r[kind + "f_rs"].at[j], s, far
        )

    def beside(kind, j, i):
        ref = landing[kind]
        block = far if i else t
        return remote(
            ref.at[j, block],
            ref.at[j, block],
            r[kind + "n_ss"].at[j, i],
            r[kind + "n_rs"].at[j, i],
            s,
            near,
        )

    def spread_out(kind, j):
        across(kind, j).start()
        beside(kind, j, 0).start()

    def pass_far(kind, j):
        with jax.named_scope(f"z_{kind}"):
            crossing(kind, (s + 1) % n, j, s).wait_recv()
        spread_out(kind, j)

    def pass_near(kind, j):
        with jax.named_scope(f"far_{kind}"):
            across(kind, j).wait()
        beside(kind, j, 1).start()

    def gathered(kind, j):
        with jax.named_scope(f"near_{kind}"):
            beside(kind, j, 0).wait()
            beside(kind, j, 1).wait()

    fetched("ids", "aff", "chance")
    ids_all = r["ids"][...]
    ids = ids_all[:, 0:rows]
    for i in range(1, tp):
        ids = jnp.where(t == i, ids_all[:, i * rows : (i + 1) * rows], ids)
    first, hit = members(ids, n, locals_)
    place = places(hit, rows)
    lift = jnp.exp(r["aff"][...])
    share = r["chance"][...] / (lift[0:1] + lift[1:2])
    slot = iota((cap, rows), 0).astype(F32)
    lane = iota((cap, EXTRA), 1)
    fetched("carry")
    carry = r["carry"][...]
    for d in range(n):
        onehot = jnp.where((place[d : d + 1] == slot) & (hit[d : d + 1] > 0.5), 1.0, 0.0)
        r["oh_own"][d] = onehot.astype(BF16)
        r["c_send"][d, :, 0:model] = jnp.dot(
            onehot.astype(BF16), carry, preferred_element_type=F32
        ).astype(BF16)
        flag = jnp.sum(onehot * first[d : d + 1], axis=1, keepdims=True)
        extra = jnp.where(lane == 2 * locals_, flag, 0.0)
        for l in range(locals_):
            expert = d * locals_ + l
            mine = share * (
                jnp.where(ids[0:1] == expert, lift[0:1], 0.0)
                + jnp.where(ids[1:2] == expert, lift[1:2], 0.0)
            )
            col = jnp.sum(onehot * mine, axis=1, keepdims=True)
            high = col.astype(BF16).astype(F32)
            extra = jnp.where(lane == 2 * l, high, extra)
            extra = jnp.where(lane == 2 * l + 1, col - high, extra)
        r["c_send"][d, :, model : model + EXTRA] = extra.astype(BF16)
    r["carr"][own, t] = r["c_send"][s]

    dispatches(0)
    spread_out("c", own)

    fetched("raw", "extra", "fade")
    dt_t = jnp.log1p(jnp.exp(r["raw"][...]))
    fade = jnp.broadcast_to(r["fade"][...], (heads, heads))
    fade = jnp.where(iota((heads, heads), 0) == iota((heads, heads), 1), fade, 0.0)
    la_t = r["extra"][...] - jnp.sum(fade, axis=1, keepdims=True) * dt_t
    row_i = iota((length, length), 0)
    col_i = iota((length, length), 1)
    lower = row_i >= col_i
    cum = last_dims(jnp.where(lower, 1.0, 0.0), la_t)
    dt = last_dims(jnp.where(row_i == col_i, 1.0, 0.0), dt_t)
    cum_t = jnp.dot(
        la_t,
        jnp.where(row_i <= col_i, 1.0, 0.0),
        precision=HIGHEST,
        preferred_element_type=F32,
    )

    ext = r["ext"]
    ext[TAIL:, 0:width] = r["x"][...].astype(F32)
    ext[TAIL:, width : width + STATE] = r["b"][...].astype(F32)
    ext[TAIL:, width + STATE : width + 2 * STATE] = r["c"][...].astype(F32)
    fetched("kx", "kb", "kc")
    ext[0:TAIL, :] = jnp.zeros((TAIL, width + 2 * STATE), F32)

    @pl.when(s > 0)
    def _():
        with jax.named_scope("tails"):
            tails.wait_recv()
        ext[0:TAIL, :] = r["tail"][...].astype(F32)

    def conv(taps, first, count):
        kernel_len = taps.shape[0]
        total = None
        for j in range(kernel_len):
            at = TAIL - kernel_len + 1 + j
            term = taps[j : j + 1, :] * ext[at : at + length, first : first + count]
            total = term if total is None else total + term
        return silu(total)

    keys = conv(r["kb"], width, STATE).astype(BF16)
    xdt = conv(r["kx"], 0, width) * spread(dt, width)
    tot = cum[length - 1 : length, :]
    remain = jnp.exp(tot - cum)
    state = first_dims(keys, (xdt * spread(remain, width)).astype(BF16))
    r["st_send"][...] = state.astype(BF16)
    r["tot_send"][...] = jnp.broadcast_to(spread(tot, width), r["tot_send"].shape)

    def total_copy(k):
        return remote(
            r["tot_send"],
            r["tot_buf"].at[k],
            r["tot_ss"].at[k - 1],
            r["tot_rs"].at[k - 1],
            (s + k) % n,
            t,
        )

    def state_copy(k):
        return remote(
            r["st_send"],
            r["st_buf"].at[k],
            r["st_ss"].at[k - 1],
            r["st_rs"].at[k - 1],
            (s + k) % n,
            t,
        )

    if n == 4:

        @pl.when(s == 2)
        def _():
            total_copy(1).start()

        @pl.when(s % 2 == 0)
        def _():
            state_copy(1).start()

    else:
        for k in range(1, n):

            @pl.when(s + k < n)
            def _(k=k):
                total_copy(k).start()
                state_copy(k).start()

    dispatches(1)

    first, hit = members(ids_all, n, locals_)
    place = places(hit, rows)
    slot_row, slot_pos = iota((slots, length), 0), iota((slots, length), 1)
    same = slot_row // cap == slot_pos // rows
    slot = (slot_row % cap).astype(F32)
    for d in range(n):
        onehot = same & (place[d : d + 1] == slot) & (hit[d : d + 1] > 0.5)
        r["oh_seg"][d] = jnp.where(onehot, 1.0, 0.0).astype(BF16)
    queries = conv(r["kc"], width + STATE, STATE).astype(BF16)
    scores = lax.dot_general(
        queries, keys, (((1,), (1,)), ((), ())), preferred_element_type=F32
    )
    xdt_b = xdt.astype(BF16)
    lane_head = iota((length, width), 1) // HEAD_DIM
    mixed = jnp.zeros((length, width), F32)
    for h in range(heads):
        between = jnp.where(lower, cum[:, h : h + 1] - cum_t[h : h + 1, :], -1e30)
        weights = (scores * jnp.exp(between)).astype(BF16)
        chosen = jnp.where(lane_head == h, xdt_b, jnp.zeros_like(xdt_b))
        mixed = mixed + jnp.dot(weights, chosen, preferred_element_type=F32)
    reach = jnp.exp(spread(cum, width))
    fetched("z")
    modulation = silu(r["z"][...].astype(F32))

    def steps(at):
        for v in range(n):
            if n == 4 and STEPS[v].get(at):

                @pl.when(s == v)
                def _(v=v):
                    for step in STEPS[v][at]:
                        if step == LAST:
                            pl.semaphore_wait(r["clear"], 2)
                            for kind, d in planned(3, v):
                                dispatch(kind, d)
                        elif step == CLEAR:
                            state_copy(1).wait_send()
                            state_copy(2).wait_send()
                            for tpi in (t, near):
                                pl.semaphore_signal(
                                    r["clear"],
                                    inc=1,
                                    device_id={"sp": s - 1, "tp": tpi},
                                    device_id_type=pl.DeviceIdType.MESH,
                                )
                        else:
                            acts[step - step % 10](step % 10)

    acts = {
        FC: functools.partial(pass_far, "c"),
        FG: functools.partial(pass_far, "g"),
        NC: functools.partial(pass_near, "c"),
        NG: functools.partial(pass_near, "g"),
    }
    steps("pre")
    incoming = r["incoming"]
    incoming[...] = jnp.zeros_like(incoming)
    if n == 4:

        @pl.when(s == 1)
        def _():
            with jax.named_scope("state"):
                state_copy(1).wait_recv()
            before = r["st_buf"][1].astype(F32)
            incoming[...] = before
            r["st_send"][...] = (before * jnp.exp(r["tot_send"][0:1, :]) + state).astype(BF16)
            state_copy(1).start()
            state_copy(2).start()

        @pl.when(s == 2)
        def _():
            with jax.named_scope("state"):
                state_copy(1).wait_recv()
            incoming[...] = r["st_buf"][1].astype(F32)

        @pl.when(s == 3)
        def _():
            with jax.named_scope("state"):
                total_copy(1).wait_recv()
                state_copy(1).wait_recv()
                state_copy(2).wait_recv()
            incoming[...] = r["st_buf"][2].astype(F32) * jnp.exp(
                r["tot_buf"][1, 0:1, :]
            ) + r["st_buf"][1].astype(F32)

    else:
        for k in range(n - 1, 0, -1):

            @pl.when(k <= s)
            def _(k=k):
                total_copy(k).wait_recv()
                state_copy(k).wait_recv()
                incoming[...] = incoming[...] * jnp.exp(r["tot_buf"][k, 0:1, :]) + r["st_buf"][
                    k
                ].astype(F32)

    outside = jnp.dot(queries, incoming[...].astype(BF16), preferred_element_type=F32)
    gated = ((mixed + outside * reach) * modulation).astype(BF16)
    for d in range(n):
        picked = jnp.dot(r["oh_seg"][d], gated, preferred_element_type=F32)
        r["g_send"][d] = picked.astype(BF16).reshape(slots, width)
    r["gbuf"][own, t] = r["g_send"][s]
    dispatches(2)
    spread_out("g", own)

    with jax.named_scope("weights"):
        fetched("gain", "sgain", "blend", "wg", "wu", "wd")

    def experts(j, between=None):
        gathered("c", j)
        gathered("g", j)
        squares = jnp.zeros((slots, 1), F32)
        for i in range(tp):
            piece = r["gbuf"][j, i].astype(F32)
            squares = squares + jnp.sum(piece * piece, axis=1, keepdims=True)
        scale = lax.rsqrt(squares / (tp * width) + EPS)
        rowsin = r["carr"][j].reshape(slots, model + EXTRA)
        projected = rowsin[:, 0:model].astype(F32)
        for i in range(tp):
            span = slice(i * width, (i + 1) * width)
            normed = (r["gbuf"][j, i].astype(F32) * scale * r["gain"][:, span]).astype(BF16)
            projected = projected + jnp.dot(
                normed, r["blend"][span, :], preferred_element_type=F32
            )
        middle = projected.astype(BF16)
        r["mid"][...] = middle.reshape(tp, cap, model)
        r["keep"][j] = r["mid"][t]
        wide = middle.astype(F32)
        tokens = (
            wide
            * lax.rsqrt(jnp.mean(wide * wide, axis=1, keepdims=True) + EPS)
            * r["sgain"][...]
        ).astype(BF16)
        lots = rowsin[:, model : model + EXTRA].astype(F32)
        total = None
        for l in range(locals_):
            part_share = lots[:, 2 * l : 2 * l + 1] + lots[:, 2 * l + 1 : 2 * l + 2]
            gate = jnp.dot(tokens, r["wg"][l], preferred_element_type=F32)
            up = jnp.dot(tokens, r["wu"][l], preferred_element_type=F32)
            hidden = (silu(gate) * up * part_share).astype(BF16)
            term = jnp.dot(hidden, r["wd"][l], preferred_element_type=F32)
            total = term if total is None else total + term
            if l == 0 and between is not None:
                between()
        r["part"][j] = total.astype(BF16).reshape(tp, cap, model)
        near_copy(j, 1).start()
        near_copy(j, 0).start()

    def near_copy(j, i):
        return remote(
            r["part"].at[j, near if i == 0 else near_far],
            r["rs1"].at[j, i],
            r["p1_ss"].at[j, i],
            r["p1_rs"].at[j, i],
            s,
            near,
        )

    def half_rows(h):
        return pl.ds(h * part_rows, part_rows)

    def far_copy(j, h):
        return remote(
            r["far_send"].at[j, half_rows(h)],
            r["rs2"].at[j, half_rows(h)],
            r["p2_ss"].at[j, h],
            r["p2_rs"].at[j, h],
            s,
            far,
        )

    def reduce_near(j):
        with jax.named_scope("p1"):
            near_copy(j, 1).wait()
            near_copy(j, 0).wait()
        for h in range(halves):
            at = half_rows(h)
            r["far_send"][j, at] = (
                r["part"][j, far, at].astype(F32) + r["rs1"][j, 1, at].astype(F32)
            ).astype(BF16)
            far_copy(j, h).start()

    def returning(j, place, h, lands):
        return remote(
            r["ret_send"].at[j, half_rows(h)],
            r["ret"].at[place, half_rows(h)],
            r["ret_ss"].at[max(j - 1, 0) if n == 4 else (source_of(j) + n - 1 - s) % n, h],
            r["ret_rs"].at[(place + n - 1 - lands) % n, h],
            source_of(j),
            t,
        )

    def reduce_far(j):
        lanes = slice(model + 2 * locals_, model + 2 * locals_ + 1)
        for h in range(halves):
            at = half_rows(h)
            with jax.named_scope("p2"):
                far_copy(j, h).wait()
            r["ret_send"][j, at] = (
                r["keep"][j, at].astype(F32) * r["carr"][j, t, at, lanes].astype(F32)
                + r["part"][j, t, at].astype(F32)
                + r["rs1"][j, 0, at].astype(F32)
                + r["rs2"][j, at].astype(F32)
            ).astype(BF16)

            @pl.when(source_of(j) != s)
            def _(h=h):
                returning(j, s, h, source_of(j)).start()

        @pl.when(source_of(j) == s)
        def _():
            r["ret"][s] = r["ret_send"][j]

    acts |= {RN: reduce_near, RF: reduce_far}
    if n == 4:
        steps("a")
        for j in range(n):
            experts(j, lambda: steps(f"m{j}"))
            steps("bcde"[j])
    else:

        def one(j, carried):
            @pl.when(j != s)
            def _():
                pass_far("c", j)
                pass_far("g", j)

            pass_near("c", j)
            pass_near("g", j)
            experts(j)
            reduce_near(j)
            reduce_far(j)
            return carried

        lax.fori_loop(0, n, one, 0)

    result = jnp.zeros((rows, model), F32)
    for d in range(n):

        @pl.when(s != d)
        def _(d=d):
            with jax.named_scope(f"ret_{d}"):
                for h in range(halves):
                    returning(1, d, h, s).wait_recv()

        result = result + first_dims(r["oh_own"][d], r["ret"][d])
    with jax.named_scope("store"):
        r["out"][...] = result.astype(BF16)

    @pl.when(s < n - 1)
    def _():
        tails.wait_send()

    for j in range(n):

        @pl.when(s != j)
        def _(j=j):
            crossing("c", j, slot_at(j)).wait_send()
            crossing("g", j, slot_at(j)).wait_send()

        @pl.when(source_of(j) != s)
        def _(j=j):
            for h in range(halves):
                returning(j, s, h, source_of(j)).wait_send()

    if n == 4:

        @pl.when(s == 2)
        def _():
            total_copy(1).wait_send()

        @pl.when(s % 2 == 0)
        def _():
            state_copy(1).wait_send()

    else:
        for k in range(1, n):

            @pl.when(s + k < n)
            def _(k=k):
                total_copy(k).wait_send()
                state_copy(k).wait_send()


INPUTS = ("x", "b", "c", "ids", "aff", "chance", "carry", "raw", "extra", "fade")
INPUTS += ("kx", "kb", "kc", "z", "gain", "sgain", "blend", "wg", "wu", "wd")


FC, FG, NC, NG, RN, RF, LAST, CLEAR = range(10, 90, 10)
C, G = 0, 10
ORDER = ((0, 1, 2, 3), (1, 0, 2, 3), (2, 0, 1, 3), (3, 2, 0, 1))
SENDS = (
    ((), (C + 2, C + 1,), (G + 1,), (G + 2, C + 3, G + 3,)),
    ((C + 2, C + 0,), (), (G + 2, C + 3, G + 3, G + 0,), ()),
    ((C + 1, C + 0, C + 3,), (), (G + 1, G + 0, G + 3,), ()),
    ((C + 2, C + 1, C + 0,), (), (G + 2, G + 1, G + 0,), ()),
)
STEPS = (
    dict(
        a=(FC + 1, NC + 0, NG + 0,),
        b=(LAST, FC + 3, NC + 1, FG + 1, FC + 2, NG + 1, FG + 2,),
        m1=(FG + 3,),
        c=(NC + 2, NC + 3, NG + 2, RN + 1,),
        m2=(NG + 3,),
        m3=(RN + 2,),
        e=(RF + 1, RN + 3, RF + 2, RN + 0, RF + 3, RF + 0,),
    ),
    dict(
        a=(CLEAR, NC + 0, FC + 3, NG + 0, FC + 2,),
        m0=(FC + 1,),
        b=(FG + 1, NC + 2, FG + 2, NC + 1, FG + 3, NG + 1,),
        m1=(NG + 2,),
        c=(NC + 3,),
        m2=(RN + 1, NG + 3,),
        m3=(RN + 2,),
        e=(RN + 3, RF + 1, RF + 2, RN + 0, RF + 3, RF + 0,),
    ),
    dict(
        pre=(FC + 2, FC + 3,),
        a=(FC + 1, NC + 2, NC + 3, NC + 0, FG + 1, NG + 0,),
        m0=(FG + 3,),
        b=(NC + 1, FG + 2, NG + 1,),
        m1=(RN + 0,),
        c=(NG + 2,),
        m2=(RN + 1, NG + 3,),
        m3=(RN + 2,),
        e=(RF + 1, RN + 3, RF + 2, RF + 3, RF + 0,),
    ),
    dict(
        pre=(FC + 1,),
        a=(NC + 1, NC + 0, FG + 1, NG + 0,),
        m0=(NG + 1, FC + 2,),
        b=(FG + 2,),
        c=(FC + 3, FG + 3, NC + 2, NG + 2,),
        m2=(RN + 1,),
        d=(NC + 3, NG + 3, RN + 2,),
        e=(RF + 1, RN + 3, RF + 2, RN + 0, RF + 3, RF + 0,),
    ),
)


def per_device(
    n,
    tp,
    carryover_vector,
    channel_source_entries,
    final_modulation_vector,
    entering_basis_matrix,
    readout_basis_matrix,
    raw_stride_amount,
    extra_log_attenuation,
    channel_fading_rate,
    channel_source_kernel,
    entering_basis_kernel,
    readout_basis_kernel,
    modulated_rescaling_vector,
    blender_final_matrix,
    specialist_rescaling_vector,
    specialist_gating_matrices,
    widening_matrices,
    contracting_matrices,
    assigned_specialist_ids,
    specialist_choice_affinity,
    cluster_chance,
):
    length, width = channel_source_entries.shape
    rows, model = carryover_vector.shape
    locals_ = specialist_gating_matrices.shape[0]
    experts = n * locals_
    picks = assigned_specialist_ids.shape[1]
    assert tp == 4 and picks == 2 and entering_basis_matrix.shape[1] == STATE
    per_expert = 2 * rows * picks // experts
    group_size = experts // EXPERT_GROUPS
    if group_size <= locals_:
        cap = locals_ * per_expert // picks
    else:
        cap = locals_ * per_expert
    cap = -(-min(cap, rows) // 16) * 16
    slots = tp * cap
    given = dict(
        ids=assigned_specialist_ids.T,
        aff=specialist_choice_affinity.T,
        chance=cluster_chance[None, :],
        carry=carryover_vector,
        raw=raw_stride_amount.T,
        extra=extra_log_attenuation.T,
        fade=channel_fading_rate[None, :],
        x=channel_source_entries,
        b=entering_basis_matrix,
        c=readout_basis_matrix,
        kx=channel_source_kernel,
        kb=entering_basis_kernel,
        kc=readout_basis_kernel,
        z=final_modulation_vector,
        gain=modulated_rescaling_vector[None, :],
        sgain=specialist_rescaling_vector[None, :],
        blend=blender_final_matrix,
        wg=specialist_gating_matrices,
        wu=widening_matrices,
        wd=contracting_matrices,
    )
    operands = [pltpu.with_memory_space_constraint(given[name], pltpu.HBM) for name in INPUTS]
    vmem = pltpu.VMEM
    dma = pltpu.SemaphoreType.DMA
    scratch = {name: vmem(given[name].shape, given[name].dtype) for name in INPUTS}
    reach = 2 if n == 4 else n - 1
    scratch |= dict(
        tail_send=vmem((TAIL, width + 2 * STATE), BF16),
        tail=vmem((TAIL, width + 2 * STATE), BF16),
        ext=vmem((TAIL + length, width + 2 * STATE), F32),
        st_send=vmem((STATE, width), BF16),
        tot_send=vmem((8, width), F32),
        st_buf=vmem((n, STATE, width), BF16),
        tot_buf=vmem((n, 8, width), F32),
        incoming=vmem((STATE, width), F32),
        oh_own=vmem((n, cap, rows), BF16),
        oh_seg=vmem((n, slots, length), BF16),
        c_send=vmem((n, cap, model + EXTRA), BF16),
        carr=vmem((n, tp, cap, model + EXTRA), BF16),
        g_send=vmem((n, slots, width), BF16),
        gbuf=vmem((n, tp, slots, width), BF16),
        mid=vmem((tp, cap, model), BF16),
        keep=vmem((n, cap, model), BF16),
        part=vmem((n, tp, cap, model), BF16),
        rs1=vmem((n, 2, cap, model), BF16),
        far_send=vmem((n, cap, model), BF16),
        rs2=vmem((n, cap, model), BF16),
        ret_send=vmem((n, cap, model), BF16),
        ret=vmem((n, cap, model), BF16),
        local_sem=dma((len(INPUTS),)),
        clear=pltpu.SemaphoreType.REGULAR,
    )
    for name, shape in dict(
        tail=(1,),
        st=(reach,),
        tot=(1 if n == 4 else reach,),
        cz=(n - 1,),
        cf=(n,),
        cn=(n, 2),
        gz=(n - 1,),
        gf=(n,),
        gn=(n, 2),
        p1=(n, 2),
        p2=(n, halves_of(cap)),
        ret=(n - 1, halves_of(cap)),
    ).items():
        scratch[name + "_ss"] = dma(shape)
        scratch[name + "_rs"] = dma(shape)
    names = [name + "_hbm" for name in INPUTS] + ["out"] + list(scratch)
    return pl.pallas_call(
        functools.partial(kernel, n, tp, cap, names),
        out_shape=pltpu.VMEM((rows, model), BF16),
        in_specs=[pl.BlockSpec(memory_space=pltpu.HBM)] * len(operands),
        out_specs=pl.BlockSpec(memory_space=pltpu.VMEM),
        scratch_shapes=list(scratch.values()),
        compiler_params=pltpu.CompilerParams(
            collective_id=0,
            has_side_effects=True,
            vmem_limit_bytes=(40 if n <= 8 else 60) * 1024 * 1024,
        ),
    )(*operands)


def solution(mesh):
    return jax.shard_map(
        functools.partial(per_device, mesh.shape["sp"], mesh.shape["tp"]),
        mesh=mesh,
        in_specs=(
            P(("grp", "sp", "tp"), None),
            P(("grp", "sp"), "tp"),
            P(("grp", "sp"), "tp"),
            P(("grp", "sp"), "tp"),
            P(("grp", "sp"), "tp"),
            P(("grp", "sp"), "tp"),
            P(("grp", "sp"), "tp"),
            P("tp"),
            P(None, "tp"),
            P(None, "tp"),
            P(None, "tp"),
            P(),
            P(),
            P(),
            P("sp", None, "tp"),
            P("sp", None, "tp"),
            P("sp", "tp", None),
            P(("grp", "sp"), None),
            P(("grp", "sp", "tp"), None),
            P(("grp", "sp", "tp")),
        ),
        out_specs=P(("grp", "sp", "tp"), None),
        check_vma=False,
    )
```

```python
import functools

import jax
import jax.numpy as jnp
from jax import lax
from jax.experimental import pallas as pl
from jax.experimental.pallas import tpu as pltpu
from jax.sharding import PartitionSpec as P

HEAD_DIM = 64
STATE = 128
EXPERT_GROUPS = 4
EPS = 1e-06
HIGHEST = lax.Precision.HIGHEST
F32 = jnp.float32
BF16 = jnp.bfloat16
TAIL = 16
EXTRA = 128


def silu(v):
    return v / (1.0 + jnp.exp(-v))


def iota(shape, dim):
    return lax.broadcasted_iota(jnp.int32, shape, dim)


def first_dims(a, b, precision=None):
    return lax.dot_general(
        a, b, (((0,), (0,)), ((), ())), precision=precision, preferred_element_type=F32
    )


def last_dims(a, b):
    return lax.dot_general(
        a, b, (((1,), (1,)), ((), ())), precision=HIGHEST, preferred_element_type=F32
    )


def spread(cols, width):
    heads = cols.shape[1]
    lane_head = iota((cols.shape[0], width), 1) // HEAD_DIM
    out = jnp.broadcast_to(cols[:, 0:1], (cols.shape[0], width))
    for h in range(1, heads):
        out = jnp.where(lane_head == h, cols[:, h : h + 1], out)
    return out


def members(ids, n, locals_):
    count = -(-n // 8) * 8
    low = iota((count, ids.shape[1]), 0) * locals_
    id0, id1 = ids[0:1], ids[1:2]
    hit0 = (id0 >= low) & (id0 < low + locals_)
    hit1 = (id1 >= low) & (id1 < low + locals_)
    return jnp.where(hit0, 1.0, 0.0), jnp.where(hit0 | hit1, 1.0, 0.0)


def places(hit, rows):
    length = hit.shape[1]
    i, j = iota((length, length), 0), iota((length, length), 1)
    earlier = jnp.where((i < j) & (i // rows == j // rows), 1.0, 0.0).astype(BF16)
    return jnp.dot(hit.astype(BF16), earlier, preferred_element_type=F32)


def halves_of(cap):
    return 2 if cap % 32 == 0 else 1


def kernel(n, tp, cap, names, *refs):
    r = dict(zip(names, refs))
    s = lax.axis_index("sp")
    t = lax.axis_index("tp")
    length, width = r["x"].shape
    rows, model = r["carry"].shape
    heads = width // HEAD_DIM
    locals_ = r["wg"].shape[0]
    slots = tp * cap
    halves = halves_of(cap)
    part_rows = cap // halves
    far = (t + tp // 2) % tp
    near = t + 1 - 2 * (t % 2)
    near_far = (near + tp // 2) % tp

    place4 = (1 + 3 * (s % 2)) * (1 + 15 * (s // 2))

    def listed(row):
        return sum(v * 4**i for i, v in enumerate(row)) // place4 % 4

    if n == 4:
        own = 0
        source = [listed([ORDER[v][j] for v in range(n)]) for j in range(n)]
    else:
        own = s
        routes = [[d for d in range(n) if d != v] for v in range(n)]

    def source_of(j):
        return source[j] if n == 4 else j

    def planned(stage, v):
        if n == 4:
            return [("c" if code < G else "g", code % 10) for code in SENDS[v][stage]]
        return [("cg"[stage // 2], d) for d in routes[v]] if stage % 2 == 0 else []

    def slot_at(d):
        return listed([ORDER[d].index(v) for v in range(n)]) if n == 4 else s

    def remote(src, dst, ssem, rsem, sp, tpi):
        return pltpu.make_async_remote_copy(
            src_ref=src,
            dst_ref=dst,
            send_sem=ssem,
            recv_sem=rsem,
            device_id={"sp": sp, "tp": tpi},
            device_id_type=pl.DeviceIdType.MESH,
        )

    barrier = pltpu.get_barrier_semaphore()
    peers = [((s + k) % n, t) for k in range(1, n)] + [(s, near), (s, far)]
    if n == 4:
        peers.append((s + 1 - 2 * (s % 2), near))
    for sp, tpi in peers:
        pl.semaphore_signal(
            barrier,
            inc=1,
            device_id={"sp": sp, "tp": tpi},
            device_id_type=pl.DeviceIdType.MESH,
        )
    fetches = {}
    for i, name in enumerate(INPUTS):
        fetches[name] = pltpu.make_async_copy(r[name + "_hbm"], r[name], r["local_sem"].at[i])
        fetches[name].start()

    def fetched(*wanted):
        for name in wanted:
            fetches[name].wait()

    fetched("x", "b", "c")

    with jax.named_scope("barrier"):
        pl.semaphore_wait(barrier, len(peers))

    tail_lanes = dict(x=(0, width), b=(width, STATE), c=(width + STATE, STATE))
    for name, (first, count) in tail_lanes.items():
        r["tail_send"][:, first : first + count] = r[name][length - TAIL :, :]
    tails = remote(
        r["tail_send"], r["tail"], r["tail_ss"].at[0], r["tail_rs"].at[0], (s + 1) % n, t
    )

    @pl.when(s < n - 1)
    def _():
        tails.start()

    landing = {"c": r["carr"], "g": r["gbuf"]}

    def crossing(kind, d, place, lands=None):
        lands = d if lands is None else lands
        return remote(
            r[kind + "_send"].at[d],
            landing[kind].at[place, t],
            r[kind + "z_ss"].at[(d + n - 1 - s) % n],
            r[kind + "z_rs"].at[place - 1 if n == 4 else (place + n - 1 - lands) % n],
            d,
            t,
        )

    def dispatch(kind, d):
        crossing(kind, d, slot_at(d)).start()

    def dispatches(stage):
        for v in range(n):
            if planned(stage, v):

                @pl.when(s == v)
                def _(v=v):
                    for kind, d in planned(stage, v):
                        dispatch(kind, d)

    def across(kind, j):
        ref = landing[kind]
        return remote(
            ref.at[j, t], ref.at[j, t], r[kind + "f_ss"].at[j], r[kind + "f_rs"].at[j], s, far
        )

    def beside(kind, j, i):
        ref = landing[kind]
        block = far if i else t
        return remote(
            ref.at[j, block],
            ref.at[j, block],
            r[kind + "n_ss"].at[j, i],
            r[kind + "n_rs"].at[j, i],
            s,
            near,
        )

    def spread_out(kind, j):
        across(kind, j).start()
        beside(kind, j, 0).start()

    def pass_far(kind, j):
        with jax.named_scope(f"z_{kind}"):
            crossing(kind, (s + 1) % n, j, s).wait_recv()
        spread_out(kind, j)

    def pass_near(kind, j):
        with jax.named_scope(f"far_{kind}"):
            across(kind, j).wait()
        beside(kind, j, 1).start()

    def gathered(kind, j):
        with jax.named_scope(f"near_{kind}"):
            beside(kind, j, 0).wait()
            beside(kind, j, 1).wait()

    fetched("ids", "aff", "chance")
    ids_all = r["ids"][...]
    ids = ids_all[:, 0:rows]
    for i in range(1, tp):
        ids = jnp.where(t == i, ids_all[:, i * rows : (i + 1) * rows], ids)
    first, hit = members(ids, n, locals_)
    place = places(hit, rows)
    lift = jnp.exp(r["aff"][...])
    share = r["chance"][...] / (lift[0:1] + lift[1:2])
    slot = iota((cap, rows), 0).astype(F32)
    lane = iota((cap, EXTRA), 1)
    fetched("carry")
    carry = r["carry"][...]
    for d in range(n):
        onehot = jnp.where((place[d : d + 1] == slot) & (hit[d : d + 1] > 0.5), 1.0, 0.0)
        r["oh_own"][d] = onehot.astype(BF16)
        r["c_send"][d, :, 0:model] = jnp.dot(
            onehot.astype(BF16), carry, preferred_element_type=F32
        ).astype(BF16)
        flag = jnp.sum(onehot * first[d : d + 1], axis=1, keepdims=True)
        extra = jnp.where(lane == 2 * locals_, flag, 0.0)
        for l in range(locals_):
            expert = d * locals_ + l
            mine = share * (
                jnp.where(ids[0:1] == expert, lift[0:1], 0.0)
                + jnp.where(ids[1:2] == expert, lift[1:2], 0.0)
            )
            col = jnp.sum(onehot * mine, axis=1, keepdims=True)
            high = col.astype(BF16).astype(F32)
            extra = jnp.where(lane == 2 * l, high, extra)
            extra = jnp.where(lane == 2 * l + 1, col - high, extra)
        r["c_send"][d, :, model : model + EXTRA] = extra.astype(BF16)
    r["carr"][own, t] = r["c_send"][s]

    dispatches(0)
    spread_out("c", own)

    fetched("raw", "extra", "fade")
    dt_t = jnp.log1p(jnp.exp(r["raw"][...]))
    fade = jnp.broadcast_to(r["fade"][...], (heads, heads))
    fade = jnp.where(iota((heads, heads), 0) == iota((heads, heads), 1), fade, 0.0)
    la_t = r["extra"][...] - jnp.sum(fade, axis=1, keepdims=True) * dt_t
    row_i = iota((length, length), 0)
    col_i = iota((length, length), 1)
    lower = row_i >= col_i
    cum = last_dims(jnp.where(lower, 1.0, 0.0), la_t)
    dt = last_dims(jnp.where(row_i == col_i, 1.0, 0.0), dt_t)
    cum_t = jnp.dot(
        la_t,
        jnp.where(row_i <= col_i, 1.0, 0.0),
        precision=HIGHEST,
        preferred_element_type=F32,
    )

    ext = r["ext"]
    ext[TAIL:, 0:width] = r["x"][...].astype(F32)
    ext[TAIL:, width : width + STATE] = r["b"][...].astype(F32)
    ext[TAIL:, width + STATE : width + 2 * STATE] = r["c"][...].astype(F32)
    fetched("kx", "kb", "kc")
    ext[0:TAIL, :] = jnp.zeros((TAIL, width + 2 * STATE), F32)

    @pl.when(s > 0)
    def _():
        with jax.named_scope("tails"):
            tails.wait_recv()
        ext[0:TAIL, :] = r["tail"][...].astype(F32)

    def conv(taps, first, count):
        kernel_len = taps.shape[0]
        total = None
        for j in range(kernel_len):
            at = TAIL - kernel_len + 1 + j
            term = taps[j : j + 1, :] * ext[at : at + length, first : first + count]
            total = term if total is None else total + term
        return silu(total)

    keys = conv(r["kb"], width, STATE).astype(BF16)
    xdt = conv(r["kx"], 0, width) * spread(dt, width)
    tot = cum[length - 1 : length, :]
    remain = jnp.exp(tot - cum)
    state = first_dims(keys, (xdt * spread(remain, width)).astype(BF16))
    r["st_send"][...] = state.astype(BF16)
    r["tot_send"][...] = jnp.broadcast_to(spread(tot, width), r["tot_send"].shape)

    def total_copy(k):
        return remote(
            r["tot_send"],
            r["tot_buf"].at[k],
            r["tot_ss"].at[k - 1],
            r["tot_rs"].at[k - 1],
            (s + k) % n,
            t,
        )

    def state_copy(k):
        return remote(
            r["st_send"],
            r["st_buf"].at[k],
            r["st_ss"].at[k - 1],
            r["st_rs"].at[k - 1],
            (s + k) % n,
            t,
        )

    if n == 4:

        @pl.when(s == 2)
        def _():
            total_copy(1).start()

        @pl.when(s % 2 == 0)
        def _():
            state_copy(1).start()

    else:
        for k in range(1, n):

            @pl.when(s + k < n)
            def _(k=k):
                total_copy(k).start()
                state_copy(k).start()

    dispatches(1)

    first, hit = members(ids_all, n, locals_)
    place = places(hit, rows)
    slot_row, slot_pos = iota((slots, length), 0), iota((slots, length), 1)
    same = slot_row // cap == slot_pos // rows
    slot = (slot_row % cap).astype(F32)
    for d in range(n):
        onehot = same & (place[d : d + 1] == slot) & (hit[d : d + 1] > 0.5)
        r["oh_seg"][d] = jnp.where(onehot, 1.0, 0.0).astype(BF16)
    queries = conv(r["kc"], width + STATE, STATE).astype(BF16)
    scores = lax.dot_general(
        queries, keys, (((1,), (1,)), ((), ())), preferred_element_type=F32
    )
    xdt_b = xdt.astype(BF16)
    lane_head = iota((length, width), 1) // HEAD_DIM
    mixed = jnp.zeros((length, width), F32)
    for h in range(heads):
        between = jnp.where(lower, cum[:, h : h + 1] - cum_t[h : h + 1, :], -1e30)
        weights = (scores * jnp.exp(between)).astype(BF16)
        chosen = jnp.where(lane_head == h, xdt_b, jnp.zeros_like(xdt_b))
        mixed = mixed + jnp.dot(weights, chosen, preferred_element_type=F32)
    reach = jnp.exp(spread(cum, width))
    fetched("z")
    modulation = silu(r["z"][...].astype(F32))

    def steps(at):
        for v in range(n):
            if n == 4 and STEPS[v].get(at):

                @pl.when(s == v)
                def _(v=v):
                    for step in STEPS[v][at]:
                        if step == LAST:
                            pl.semaphore_wait(r["clear"], 2)
                            for kind, d in planned(3, v):
                                dispatch(kind, d)
                        elif step == CLEAR:
                            state_copy(1).wait_send()
                            state_copy(2).wait_send()
                            for tpi in (t, near):
                                pl.semaphore_signal(
                                    r["clear"],
                                    inc=1,
                                    device_id={"sp": s - 1, "tp": tpi},
                                    device_id_type=pl.DeviceIdType.MESH,
                                )
                        else:
                            acts[step - step % 10](step % 10)

    acts = {
        FC: functools.partial(pass_far, "c"),
        FG: functools.partial(pass_far, "g"),
        NC: functools.partial(pass_near, "c"),
        NG: functools.partial(pass_near, "g"),
    }
    steps("pre")
    incoming = r["incoming"]
    incoming[...] = jnp.zeros_like(incoming)
    if n == 4:

        @pl.when(s == 1)
        def _():
            with jax.named_scope("state"):
                state_copy(1).wait_recv()
            before = r["st_buf"][1].astype(F32)
            incoming[...] = before
            r["st_send"][...] = (before * jnp.exp(r["tot_send"][0:1, :]) + state).astype(BF16)
            state_copy(1).start()
            state_copy(2).start()

        @pl.when(s == 2)
        def _():
            with jax.named_scope("state"):
                state_copy(1).wait_recv()
            incoming[...] = r["st_buf"][1].astype(F32)

        @pl.when(s == 3)
        def _():
            with jax.named_scope("state"):
                total_copy(1).wait_recv()
                state_copy(1).wait_recv()
                state_copy(2).wait_recv()
            incoming[...] = r["st_buf"][2].astype(F32) * jnp.exp(
                r["tot_buf"][1, 0:1, :]
            ) + r["st_buf"][1].astype(F32)

    else:
        for k in range(n - 1, 0, -1):

            @pl.when(k <= s)
            def _(k=k):
                total_copy(k).wait_recv()
                state_copy(k).wait_recv()
                incoming[...] = incoming[...] * jnp.exp(r["tot_buf"][k, 0:1, :]) + r["st_buf"][
                    k
                ].astype(F32)

    outside = jnp.dot(queries, incoming[...].astype(BF16), preferred_element_type=F32)
    gated = ((mixed + outside * reach) * modulation).astype(BF16)
    for d in range(n):
        picked = jnp.dot(r["oh_seg"][d], gated, preferred_element_type=F32)
        r["g_send"][d] = picked.astype(BF16).reshape(slots, width)
    r["gbuf"][own, t] = r["g_send"][s]
    dispatches(2)
    spread_out("g", own)

    with jax.named_scope("weights"):
        fetched("gain", "sgain", "blend", "wg", "wu", "wd")

    def experts(j, between=None):
        gathered("c", j)
        gathered("g", j)
        squares = jnp.zeros((slots, 1), F32)
        for i in range(tp):
            piece = r["gbuf"][j, i].astype(F32)
            squares = squares + jnp.sum(piece * piece, axis=1, keepdims=True)
        scale = lax.rsqrt(squares / (tp * width) + EPS)
        rowsin = r["carr"][j].reshape(slots, model + EXTRA)
        projected = rowsin[:, 0:model].astype(F32)
        for i in range(tp):
            span = slice(i * width, (i + 1) * width)
            normed = (r["gbuf"][j, i].astype(F32) * scale * r["gain"][:, span]).astype(BF16)
            projected = projected + jnp.dot(
                normed, r["blend"][span, :], preferred_element_type=F32
            )
        middle = projected.astype(BF16)
        r["mid"][...] = middle.reshape(tp, cap, model)
        r["keep"][j] = r["mid"][t]
        wide = middle.astype(F32)
        tokens = (
            wide
            * lax.rsqrt(jnp.mean(wide * wide, axis=1, keepdims=True) + EPS)
            * r["sgain"][...]
        ).astype(BF16)
        lots = rowsin[:, model : model + EXTRA].astype(F32)
        total = None
        for l in range(locals_):
            part_share = lots[:, 2 * l : 2 * l + 1] + lots[:, 2 * l + 1 : 2 * l + 2]
            gate = jnp.dot(tokens, r["wg"][l], preferred_element_type=F32)
            up = jnp.dot(tokens, r["wu"][l], preferred_element_type=F32)
            hidden = (silu(gate) * up * part_share).astype(BF16)
            term = jnp.dot(hidden, r["wd"][l], preferred_element_type=F32)
            total = term if total is None else total + term
            if l == 0 and between is not None:
                between()
        r["part"][j] = total.astype(BF16).reshape(tp, cap, model)
        near_copy(j, 1).start()
        near_copy(j, 0).start()

    def near_copy(j, i):
        return remote(
            r["part"].at[j, near if i == 0 else near_far],
            r["rs1"].at[j, i],
            r["p1_ss"].at[j, i],
            r["p1_rs"].at[j, i],
            s,
            near,
        )

    def half_rows(h):
        return pl.ds(h * part_rows, part_rows)

    def far_copy(j, h):
        return remote(
            r["far_send"].at[j, half_rows(h)],
            r["rs2"].at[j, half_rows(h)],
            r["p2_ss"].at[j, h],
            r["p2_rs"].at[j, h],
            s,
            far,
        )

    def reduce_near(j):
        with jax.named_scope("p1"):
            near_copy(j, 1).wait()
            near_copy(j, 0).wait()
        for h in range(halves):
            at = half_rows(h)
            r["far_send"][j, at] = (
                r["part"][j, far, at].astype(F32) + r["rs1"][j, 1, at].astype(F32)
            ).astype(BF16)
            far_copy(j, h).start()

    def returning(j, place, h, lands):
        return remote(
            r["ret_send"].at[j, half_rows(h)],
            r["ret"].at[place, half_rows(h)],
            r["ret_ss"].at[max(j - 1, 0) if n == 4 else (source_of(j) + n - 1 - s) % n, h],
            r["ret_rs"].at[(place + n - 1 - lands) % n, h],
            source_of(j),
            t,
        )

    def reduce_far(j):
        lanes = slice(model + 2 * locals_, model + 2 * locals_ + 1)
        for h in range(halves):
            at = half_rows(h)
            with jax.named_scope("p2"):
                far_copy(j, h).wait()
            r["ret_send"][j, at] = (
                r["keep"][j, at].astype(F32) * r["carr"][j, t, at, lanes].astype(F32)
                + r["part"][j, t, at].astype(F32)
                + r["rs1"][j, 0, at].astype(F32)
                + r["rs2"][j, at].astype(F32)
            ).astype(BF16)

            @pl.when(source_of(j) != s)
            def _(h=h):
                returning(j, s, h, source_of(j)).start()

        @pl.when(source_of(j) == s)
        def _():
            r["ret"][s] = r["ret_send"][j]

    acts |= {RN: reduce_near, RF: reduce_far}
    if n == 4:
        steps("a")
        for j in range(n):
            experts(j, lambda: steps(f"m{j}"))
            steps("bcde"[j])
    else:

        def one(j, carried):
            @pl.when(j != s)
            def _():
                pass_far("c", j)
                pass_far("g", j)

            pass_near("c", j)
            pass_near("g", j)
            experts(j)
            reduce_near(j)
            reduce_far(j)
            return carried

        lax.fori_loop(0, n, one, 0)

    result = jnp.zeros((rows, model), F32)
    for d in range(n):

        @pl.when(s != d)
        def _(d=d):
            with jax.named_scope(f"ret_{d}"):
                for h in range(halves):
                    returning(1, d, h, s).wait_recv()

        result = result + first_dims(r["oh_own"][d], r["ret"][d])
    with jax.named_scope("store"):
        r["out"][...] = result.astype(BF16)

    @pl.when(s < n - 1)
    def _():
        tails.wait_send()

    for j in range(n):

        @pl.when(s != j)
        def _(j=j):
            crossing("c", j, slot_at(j)).wait_send()
            crossing("g", j, slot_at(j)).wait_send()

        @pl.when(source_of(j) != s)
        def _(j=j):
            for h in range(halves):
                returning(j, s, h, source_of(j)).wait_send()

    if n == 4:

        @pl.when(s == 2)
        def _():
            total_copy(1).wait_send()

        @pl.when(s % 2 == 0)
        def _():
            state_copy(1).wait_send()

    else:
        for k in range(1, n):

            @pl.when(s + k < n)
            def _(k=k):
                total_copy(k).wait_send()
                state_copy(k).wait_send()


INPUTS = ("x", "b", "c", "ids", "aff", "chance", "carry", "raw", "extra", "fade")
INPUTS += ("kx", "kb", "kc", "z", "gain", "sgain", "blend", "wg", "wu", "wd")


FC, FG, NC, NG, RN, RF, LAST, CLEAR = range(10, 90, 10)
C, G = 0, 10
ORDER = ((0, 1, 2, 3), (1, 0, 2, 3), (2, 0, 1, 3), (3, 2, 0, 1))
SENDS = (
    ((), (C + 2, C + 1,), (G + 1,), (G + 2, C + 3, G + 3,)),
    ((C + 2, C + 0,), (), (G + 2, C + 3, G + 3, G + 0,), ()),
    ((C + 1, C + 0, C + 3,), (), (G + 0, G + 1, G + 3,), ()),
    ((C + 2, C + 1, C + 0,), (), (G + 2, G + 1, G + 0,), ()),
)
STEPS = (
    dict(
        a=(FC + 1, NC + 0, NG + 0,),
        b=(LAST, FC + 3, NC + 1, FG + 1, FC + 2, FG + 2, NG + 1,),
        m1=(FG + 3, NC + 2,),
        c=(NC + 3, NG + 2,),
        m2=(RN + 1, NG + 3,),
        m3=(RN + 2,),
        e=(RF + 1, RN + 3, RF + 2, RN + 0, RF + 3, RF + 0,),
    ),
    dict(
        a=(CLEAR, NC + 0, FC + 3, NG + 0, FC + 2,),
        m0=(FC + 1,),
        b=(FG + 1, NC + 2, FG + 2, NC + 1, FG + 3, NG + 1,),
        m1=(NG + 2,),
        c=(NC + 3,),
        m2=(RN + 1, NG + 3,),
        m3=(RN + 2,),
        e=(RN + 3, RF + 1, RF + 2, RN + 0, RF + 3, RF + 0,),
    ),
    dict(
        pre=(FC + 2, FC + 3,),
        a=(FC + 1, NC + 2, NC + 3, NC + 0, FG + 1, NG + 0,),
        m0=(FG + 3,),
        b=(NC + 1, FG + 2, NG + 1,),
        m1=(RN + 0,),
        c=(NG + 2,),
        m2=(RN + 1, NG + 3,),
        m3=(RN + 2,),
        e=(RF + 1, RN + 3, RF + 2, RF + 3, RF + 0,),
    ),
    dict(
        pre=(FC + 1,),
        a=(NC + 1, NC + 0, FG + 1, NG + 0,),
        m0=(NG + 1, FC + 2,),
        b=(FG + 2,),
        c=(FC + 3, FG + 3, NC + 2, NG + 2,),
        m2=(RN + 1,),
        d=(NC + 3, NG + 3, RN + 2,),
        e=(RF + 1, RN + 3, RF + 2, RN + 0, RF + 3, RF + 0,),
    ),
)


def per_device(
    n,
    tp,
    carryover_vector,
    channel_source_entries,
    final_modulation_vector,
    entering_basis_matrix,
    readout_basis_matrix,
    raw_stride_amount,
    extra_log_attenuation,
    channel_fading_rate,
    channel_source_kernel,
    entering_basis_kernel,
    readout_basis_kernel,
    modulated_rescaling_vector,
    blender_final_matrix,
    specialist_rescaling_vector,
    specialist_gating_matrices,
    widening_matrices,
    contracting_matrices,
    assigned_specialist_ids,
    specialist_choice_affinity,
    cluster_chance,
):
    length, width = channel_source_entries.shape
    rows, model = carryover_vector.shape
    locals_ = specialist_gating_matrices.shape[0]
    experts = n * locals_
    picks = assigned_specialist_ids.shape[1]
    assert tp == 4 and picks == 2 and entering_basis_matrix.shape[1] == STATE
    per_expert = 2 * rows * picks // experts
    group_size = experts // EXPERT_GROUPS
    if group_size <= locals_:
        cap = locals_ * per_expert // picks
    else:
        cap = locals_ * per_expert
    cap = -(-min(cap, rows) // 16) * 16
    slots = tp * cap
    given = dict(
        ids=assigned_specialist_ids.T,
        aff=specialist_choice_affinity.T,
        chance=cluster_chance[None, :],
        carry=carryover_vector,
        raw=raw_stride_amount.T,
        extra=extra_log_attenuation.T,
        fade=channel_fading_rate[None, :],
        x=channel_source_entries,
        b=entering_basis_matrix,
        c=readout_basis_matrix,
        kx=channel_source_kernel,
        kb=entering_basis_kernel,
        kc=readout_basis_kernel,
        z=final_modulation_vector,
        gain=modulated_rescaling_vector[None, :],
        sgain=specialist_rescaling_vector[None, :],
        blend=blender_final_matrix,
        wg=specialist_gating_matrices,
        wu=widening_matrices,
        wd=contracting_matrices,
    )
    operands = [pltpu.with_memory_space_constraint(given[name], pltpu.HBM) for name in INPUTS]
    vmem = pltpu.VMEM
    dma = pltpu.SemaphoreType.DMA
    scratch = {name: vmem(given[name].shape, given[name].dtype) for name in INPUTS}
    reach = 2 if n == 4 else n - 1
    scratch |= dict(
        tail_send=vmem((TAIL, width + 2 * STATE), BF16),
        tail=vmem((TAIL, width + 2 * STATE), BF16),
        ext=vmem((TAIL + length, width + 2 * STATE), F32),
        st_send=vmem((STATE, width), BF16),
        tot_send=vmem((8, width), F32),
        st_buf=vmem((n, STATE, width), BF16),
        tot_buf=vmem((n, 8, width), F32),
        incoming=vmem((STATE, width), F32),
        oh_own=vmem((n, cap, rows), BF16),
        oh_seg=vmem((n, slots, length), BF16),
        c_send=vmem((n, cap, model + EXTRA), BF16),
        carr=vmem((n, tp, cap, model + EXTRA), BF16),
        g_send=vmem((n, slots, width), BF16),
        gbuf=vmem((n, tp, slots, width), BF16),
        mid=vmem((tp, cap, model), BF16),
        keep=vmem((n, cap, model), BF16),
        part=vmem((n, tp, cap, model), BF16),
        rs1=vmem((n, 2, cap, model), BF16),
        far_send=vmem((n, cap, model), BF16),
        rs2=vmem((n, cap, model), BF16),
        ret_send=vmem((n, cap, model), BF16),
        ret=vmem((n, cap, model), BF16),
        local_sem=dma((len(INPUTS),)),
        clear=pltpu.SemaphoreType.REGULAR,
    )
    for name, shape in dict(
        tail=(1,),
        st=(reach,),
        tot=(1 if n == 4 else reach,),
        cz=(n - 1,),
        cf=(n,),
        cn=(n, 2),
        gz=(n - 1,),
        gf=(n,),
        gn=(n, 2),
        p1=(n, 2),
        p2=(n, halves_of(cap)),
        ret=(n - 1, halves_of(cap)),
    ).items():
        scratch[name + "_ss"] = dma(shape)
        scratch[name + "_rs"] = dma(shape)
    names = [name + "_hbm" for name in INPUTS] + ["out"] + list(scratch)
    return pl.pallas_call(
        functools.partial(kernel, n, tp, cap, names),
        out_shape=pltpu.VMEM((rows, model), BF16),
        in_specs=[pl.BlockSpec(memory_space=pltpu.HBM)] * len(operands),
        out_specs=pl.BlockSpec(memory_space=pltpu.VMEM),
        scratch_shapes=list(scratch.values()),
        compiler_params=pltpu.CompilerParams(
            collective_id=0,
            has_side_effects=True,
            vmem_limit_bytes=(40 if n <= 8 else 60) * 1024 * 1024,
        ),
    )(*operands)


def solution(mesh):
    return jax.shard_map(
        functools.partial(per_device, mesh.shape["sp"], mesh.shape["tp"]),
        mesh=mesh,
        in_specs=(
            P(("grp", "sp", "tp"), None),
            P(("grp", "sp"), "tp"),
            P(("grp", "sp"), "tp"),
            P(("grp", "sp"), "tp"),
            P(("grp", "sp"), "tp"),
            P(("grp", "sp"), "tp"),
            P(("grp", "sp"), "tp"),
            P("tp"),
            P(None, "tp"),
            P(None, "tp"),
            P(None, "tp"),
            P(),
            P(),
            P(),
            P("sp", None, "tp"),
            P("sp", None, "tp"),
            P("sp", "tp", None),
            P(("grp", "sp"), None),
            P(("grp", "sp", "tp"), None),
            P(("grp", "sp", "tp")),
        ),
        out_specs=P(("grp", "sp", "tp"), None),
        check_vma=False,
    )
```
